32 devices in a mesh: fs: 8 (over z, y), tp: 4 (over x, core).
Axes of the slice: x: 2, y: 2, z: 4, core: 2. Of those that a mesh axis runs over, the one named last changes fastest.
Arguments:
- prompt_tokens: bfloat16 [4, 128, 4096], P('tp'), may hold values from -6 to 6
- trained_up: float32 [4096, 16384], P('fs', 'tp'), may hold values from -0.09375 to 0.09375
- trained_down: float32 [16384, 4096], P('fs', 'tp'), may hold values from -0.046875 to 0.046875
- pre_gain: float32 [4096], P('fs'), may hold values from 0.1 to 1.9
- post_gain: float32 [4096], replicated, may hold values from 0.1 to 1.9
Outputs:
- layer_out: bfloat16 [4, 128, 4096], P('tp', 'fs')
- sampler_up: bfloat16 [4096, 16384], P(None, 'fs')
- sampler_down: bfloat16 [16384, 4096], P('fs')
The draws below stay inside these ranges and needn't reach their ends.
All inputs are finite; a program needn't handle non-finite values.
Results may differ from the reference program's by a relative error of at most 0.0081.
Values may be sent and summed in bfloat16 or wider, within the bound.
A program may use at most 128 MiB of HBM per device.

```python
import jax
import jax.numpy as jnp
from jax import lax

D = 4096
FF = 16384
TOK_G = 128
N_TP = 4


def steps_of(rng, dims, pieces, least, top_value):
    factor_of = 1.0
    for position, shards_of in pieces:
        heights = jax.random.uniform(jax.random.fold_in(jax.random.fold_in(rng, 6), position), (shards_of,), jnp.float32, least / len(pieces), top_value / len(pieces))
        factor_of = factor_of * jnp.repeat(jnp.exp(heights), dims[position] // shards_of).reshape((-1,) + (1,) * (len(dims) - 1 - position))
    return factor_of


def gaussian(own_key, shape, scale, reach, cuts=(), held_as=jnp.bfloat16):
    values = jax.random.normal(own_key, shape, jnp.float32) * scale
    if len(cuts) > 0:
        values = steps_of(own_key, shape, cuts, -0.22, 0.18) * values
    return jnp.clip(values, min=-reach, max=reach).astype(held_as)


def setup_inputs(seed: int = 0) -> dict:
    keys = jax.random.split(jax.random.key(seed), 6)
    return {
        "prompt_tokens": gaussian(keys[0], (N_TP, TOK_G, D), 1.0, 6.0, ((0, 4),)),
        "trained_up": gaussian(keys[1], (D, FF), D ** -0.5, 0.09375, ((0, 8), (1, 4)), jnp.float32),
        "trained_down": gaussian(keys[2], (FF, D), FF ** -0.5, 0.046875, ((0, 8), (1, 4)), jnp.float32),
        "pre_gain": jnp.clip(1.0 + 0.18 * jax.random.normal(keys[3], (D,), jnp.float32), 0.1, 1.9),
        "post_gain": jnp.clip(1.0 + 0.18 * jax.random.normal(keys[4], (D,), jnp.float32), 0.1, 1.9),
    }


def row_norm(values):
    return values * lax.rsqrt(lax.optimization_barrier(jnp.mean(values * values, axis=-1, keepdims=True)) + 1e-06)

def reference(prompt_tokens, trained_up, trained_down, pre_gain, post_gain):
    sampler_up = (pre_gain[:, None] * trained_up).astype(jnp.bfloat16)
    sampler_down = trained_down.astype(jnp.bfloat16)
    flat = prompt_tokens.reshape(-1, prompt_tokens.shape[-1]).astype(jnp.float32)
    normed = row_norm(flat).astype(jnp.bfloat16)
    upward = jnp.dot(normed, sampler_up, preferred_element_type=jnp.float32)
    hidden = jnp.square(jax.nn.relu(upward)).astype(jnp.bfloat16)
    summed = jnp.dot(hidden, sampler_down, preferred_element_type=jnp.float32)
    layer_out = (row_norm(summed) * post_gain).astype(jnp.bfloat16)
    return (layer_out.reshape(prompt_tokens.shape), sampler_up, sampler_down)
```

```python
import functools

import jax
import jax.numpy as jnp
from jax import lax
from jax.experimental import pallas as pl
from jax.experimental.pallas import tpu as pltpu
from jax.sharding import PartitionSpec as P

MESH = pl.DeviceIdType.MESH
EPS = 1e-06
CHUNK = 256
SEGMENTS = 4
GROUP = 4


def remote(src, dst, send_sem, recv_sem, device):
    return pltpu.make_async_remote_copy(
        src_ref=src, dst_ref=dst, send_sem=send_sem, recv_sem=recv_sem, device_id=device, device_id_type=MESH
    )


def greet(device):
    pl.semaphore_signal(pltpu.get_barrier_semaphore(), inc=1, device_id=device, device_id_type=MESH)


def loop(count, body):
    lax.fori_loop(0, count, lambda i, c: (body(i), c)[1], 0)


def span(i, size):
    return pl.ds(pl.multiple_of(i * size, size), size)


def square_norm(values):
    return values * lax.rsqrt(jnp.mean(values * values, axis=-1, keepdims=True) + EPS)


def spread_kernel(
    n_fs, n_tp, w, fused,
    up_in, down_in, tokens, gain, post, held_up, held_down, out,
    stage, dstage, upb, xup, gcol, normed, acc, hid, pacc, us, ds_in,
    xs, xr, ps, pr, ws, wr, ns, nr, ds, dr, vs, vr, *reduce_refs,
):
    f, t = lax.axis_index("fs"), lax.axis_index("tp")
    far = lax.rem(t + n_tp // 2, n_tp)
    near = t + 1 - 2 * lax.rem(t, 2)
    near_far = lax.rem(near + n_tp // 2, n_tp)
    m = n_fs // n_tp
    rows, cols = up_in.shape
    owned = cols // m
    d_rows, d_width = down_in.shape
    width = n_tp * d_width
    n_c = owned // w
    d_part = d_rows // n_c
    pieces = m * n_c
    block_of_f = f // m
    active = lax.rem(lax.rem(block_of_f, 2) + lax.rem(t, 2), 2) == 0

    def load_up(k):
        return pltpu.make_async_copy(
            up_in.at[:, span(lax.rem(k, m) * n_c + k // m, w)], stage.at[k], us.at[k]
        )

    def load_down(c):
        return pltpu.make_async_copy(down_in.at[span(c, d_part)], dstage.at[lax.rem(c, 2)], ds_in.at[lax.rem(c, 2)])

    def landed(source, c):
        return held_up.at[span(source, rows), span(c, w)]

    def x_copy(k):
        return remote(upb.at[k], xup.at[k], xs.at[k], xr.at[k], {"tp": far})

    def owner(phase, k):
        return (t if phase == 0 else far) * m + lax.rem(k, m)

    def peer_copy(phase, k):
        held = upb if phase == 0 else xup
        return remote(held.at[k], landed(f, k // m), ps.at[phase, k], pr.at[f, k // m], {"fs": owner(phase, k)})

    def start_peer(phase, k):
        @pl.when(owner(phase, k) != f)
        def _():
            peer_copy(phase, k).start()

    def end_peer(phase, k):
        @pl.when(owner(phase, k) != f)
        def _():
            peer_copy(phase, k).wait_send()

    def block(c, which):
        return held_down.at[span(c, d_part), span(which, d_width)]

    def d_copy(c):
        return remote(block(c, t), block(c, t), ds.at[c], dr.at[c], {"tp": far})

    def d_pass(c, which):
        return remote(block(c, which), block(c, which), vs.at[c], vr.at[c], {"tp": near})

    def column(which):
        return held_down.at[:, span(which, d_width)]

    def to_near(which):
        return remote(column(which), column(which), ns, nr, {"tp": near})

    def share(src, source, c):
        return remote(src, landed(source, c), ws.at[source, c], wr.at[source, c], {"tp": near})

    loop(n_fs - 1, lambda i: greet({"fs": lax.rem(f + 1 + i, n_fs)}))
    greet({"tp": far})
    greet({"tp": near})
    loop(pieces, lambda k: load_up(k).start())
    for c in range(min(2, n_c)):
        load_down(c).start()

    side = min(rows, 128)
    eye = lax.broadcasted_iota(jnp.int32, (side, side), 0) == lax.broadcasted_iota(jnp.int32, (side, side), 1)
    for b in range(rows // side):
        line = jnp.broadcast_to(gain[:, b * side : (b + 1) * side], (side, side))
        scale = jnp.sum(jnp.where(eye, line, 0.0), axis=1, keepdims=True)
        gcol[b * side : (b + 1) * side, :] = jnp.broadcast_to(scale, (side, 128))

    def convert(k):
        load_up(k).wait()
        for j in range(0, w, 128):
            upb[k, :, j : j + 128] = (gcol[...] * stage[k, :, j : j + 128]).astype(upb.dtype)

    def send(k):
        x_copy(k).start()
        start_peer(0, k)

    convert(0)
    pl.semaphore_wait(pltpu.get_barrier_semaphore(), n_fs + 1)

    def convert_and_send(k):
        convert(k)
        send(k - 1)

    lax.fori_loop(1, pieces, lambda k, c: (convert_and_send(k), c)[1], 0)
    pacc[...] = jnp.zeros_like(pacc)
    send(pieces - 1)

    def convert_down(c):
        load_down(c).wait()
        held_down[span(c, d_part), span(t, d_width)] = dstage[lax.rem(c, 2)].astype(held_down.dtype)

        @pl.when(c + 2 < n_c)
        def _():
            load_down(c + 2).start()

    def pass_on(k):
        @pl.when(k == max(pieces - 2, 0))
        def _():
            loop(n_c, lambda c: d_copy(c).start())
            to_near(t).start()

        x_copy(k).wait_recv()
        start_peer(1, k)

        @pl.when(k < n_c)
        def _():
            convert_down(k)

        @pl.when(k == n_c)
        def _():
            scaled = square_norm(tokens[...].astype(jnp.float32)).astype(jnp.bfloat16)
            for i in range(n_fs):
                normed[i] = scaled[:, i * rows : (i + 1) * rows]

    loop(pieces, pass_on)

    def gather(c):
        remote(block(c, far), block(c, far), ds.at[c], dr.at[c], {"tp": far}).wait_recv()
        d_pass(c, far).start()
        acc[...] = jnp.zeros_like(acc)

        def one(source):
            def keep_own(held):
                k = c * m + lax.rem(f, m)
                share(held.at[k], source, c).start()
                held_up[span(source, rows), span(c, w)] = held[k]

            @pl.when(jnp.logical_and(active, source == f))
            def _():
                @pl.when(block_of_f == t)
                def _():
                    keep_own(upb)

                @pl.when(block_of_f != t)
                def _():
                    keep_own(xup)

            @pl.when(jnp.logical_and(active, source != f))
            def _():
                remote(landed(source, c), landed(source, c), ws.at[source, c], pr.at[source, c], {"tp": near}).wait_recv()
                share(landed(source, c), source, c).start()

            @pl.when(jnp.logical_not(active))
            def _():
                share(landed(source, c), source, c).wait_recv()

            acc[...] += jnp.dot(
                normed[source], held_up[span(source, rows), span(c, w)], preferred_element_type=jnp.float32
            )

        loop(n_fs, one)
        hid[...] = jnp.square(jnp.maximum(acc[...], 0.0)).astype(jnp.bfloat16)
        d_pass(c, near_far).wait_recv()

        @pl.when(c == 0)
        def _():
            to_near(near).wait_recv()

    def add_down(c, first, count):
        tile = min(d_width, 512)

        def one(i):
            at = pl.ds(pl.multiple_of(first + i * tile, tile), tile)
            pacc[:, at] += jnp.dot(hid[...], held_down[span(c, d_part), at], preferred_element_type=jnp.float32)

        loop(count // tile, one)

    def whole_chunk(c):
        gather(c)
        add_down(c, 0, width)

    last = n_c - 1
    loop(last, whole_chunk)
    gather(last)
    if fused:
        sb, land, sb2, land2, fin, ss, rs, ss2, rs2 = reduce_refs
        _, q, n_o, part, seg = sb.shape
        i, o = lax.rem(f, q), f // q

        def peer(d):
            return lax.rem(i + d, q)

        def across(d):
            return lax.rem(o + d, n_o)

        def first_copy(s, d):
            return remote(sb.at[s, peer(d)], land.at[s, i], ss.at[s, d], rs.at[s, i], {"fs": o * q + peer(d)})

        def second_copy(s, d):
            return remote(sb2.at[s, across(d)], land2.at[s, o], ss2.at[s, d], rs2.at[s, o], {"fs": across(d) * q + i})

        for s in range(SEGMENTS):
            add_down(last, s * seg, seg)
            for b in range(n_o * q):
                sb[s, b % q, b // q] = pacc[b * part : (b + 1) * part, s * seg : (s + 1) * seg].astype(sb.dtype)
            for d in range(1, q):
                first_copy(s, d).start()

        for s in range(SEGMENTS):
            for d in range(1, q):
                remote(land.at[s, peer(d)], land.at[s, peer(d)], ss.at[s, d], rs.at[s, peer(d)], {"fs": f}).wait_recv()

            def total(to):
                value = pacc[span(to * q + i, part), s * seg : (s + 1) * seg]
                for d in range(1, q):
                    value += land[s, peer(d), to].astype(jnp.float32)
                return value

            for d in range(1, n_o):
                sb2[s, across(d)] = total(across(d)).astype(sb2.dtype)
            fin[:, s * seg : (s + 1) * seg] = total(o)
            for d in range(1, n_o):
                second_copy(s, d).start()

        for s in range(SEGMENTS):
            value = fin[:, s * seg : (s + 1) * seg]
            for d in range(1, n_o):
                remote(land2.at[s, across(d)], land2.at[s, across(d)], ss2.at[s, d], rs2.at[s, across(d)], {"fs": f}).wait_recv()
                value += land2[s, across(d)].astype(jnp.float32)
            fin[:, s * seg : (s + 1) * seg] = value
        total_sum = fin[...]
        scale = lax.rsqrt(jnp.mean(total_sum * total_sum, axis=-1, keepdims=True) + EPS)
        out[...] = (total_sum * scale * post[...]).astype(out.dtype)
        for s in range(SEGMENTS):
            for d in range(1, q):
                first_copy(s, d).wait_send()
            for d in range(1, n_o):
                second_copy(s, d).wait_send()
    else:
        add_down(last, 0, width)
        out[...] = pacc[...].astype(out.dtype)

    def ended(i):
        @pl.when(active)
        def _():
            source, c = i // n_c, lax.rem(i, n_c)
            share(landed(source, c), source, c).wait_send()

    loop(n_fs * n_c, ended)
    to_near(t).wait_send()

    def ended_down(c):
        d_copy(c).wait_send()
        d_pass(c, far).wait_send()

    loop(n_c, ended_down)

    def ended_pieces(k):
        x_copy(k).wait_send()
        end_peer(0, k)
        end_peer(1, k)

    loop(pieces, ended_pieces)


def sum_kernel(n_fs, parts, gain, out, land, ss, rs):
    f = lax.axis_index("fs")

    def peer_of(i):
        return lax.rem(f + 1 + i, n_fs)

    loop(n_fs - 1, lambda i: greet({"fs": peer_of(i)}))
    pl.semaphore_wait(pltpu.get_barrier_semaphore(), n_fs - 1)

    def send(i):
        return remote(parts.at[peer_of(i)], land.at[f], ss.at[i], rs.at[f], {"fs": peer_of(i)})

    loop(n_fs - 1, lambda i: send(i).start())

    def add(i, total):
        source = peer_of(i)
        remote(land.at[source], land.at[source], ss.at[i], rs.at[source], {"fs": source}).wait_recv()
        return total + land[source].astype(jnp.float32)

    summed = lax.fori_loop(0, n_fs - 1, add, parts[f].astype(jnp.float32))
    scale = lax.rsqrt(jnp.mean(summed * summed, axis=-1, keepdims=True) + EPS)
    out[...] = (summed * scale * gain[...]).astype(out.dtype)
    loop(n_fs - 1, lambda i: send(i).wait_send())


def on_device(n_fs, n_tp, prompt_tokens, trained_up, trained_down, pre_gain, post_gain):
    bf16, f32 = jnp.bfloat16, jnp.float32
    rows, cols = trained_up.shape
    d_rows, d_cols = trained_down.shape
    tokens, width = prompt_tokens.shape[1:]
    m = n_fs // n_tp
    owned = cols // m
    w = min(owned, CHUNK)
    n_c = owned // w
    pieces = m * n_c
    share = tokens // n_fs
    q = GROUP
    n_o = n_fs // q
    seg = width // SEGMENTS
    fused = share % 16 == 0 and n_fs % q == 0 and n_o > 1
    anywhere = pl.BlockSpec(memory_space=pl.ANY)
    vmem = pl.BlockSpec(memory_space=pltpu.VMEM)
    dma = pltpu.SemaphoreType.DMA
    reduce_scratch = [
        pltpu.VMEM((SEGMENTS, q, n_o, share, seg), bf16),
        pltpu.VMEM((SEGMENTS, q, n_o, share, seg), bf16),
        pltpu.VMEM((SEGMENTS, n_o, share, seg), bf16),
        pltpu.VMEM((SEGMENTS, n_o, share, seg), bf16),
        pltpu.VMEM((share, width), f32),
        dma((SEGMENTS, q)), dma((SEGMENTS, q)),
        dma((SEGMENTS, n_o)), dma((SEGMENTS, n_o)),
    ]
    sampler_up, sampler_down, result = pl.pallas_call(
        functools.partial(spread_kernel, n_fs, n_tp, w, fused),
        out_shape=(
            pltpu.VMEM((n_fs * rows, owned), bf16),
            pltpu.VMEM((d_rows, n_tp * d_cols), bf16),
            jax.ShapeDtypeStruct((share if fused else tokens, width), bf16),
        ),
        in_specs=[anywhere, anywhere, vmem, vmem, vmem],
        out_specs=(vmem, vmem, vmem),
        scratch_shapes=[
            pltpu.VMEM((pieces, rows, w), f32),
            pltpu.VMEM((2, d_rows // n_c, d_cols), f32),
            pltpu.VMEM((pieces, rows, w), bf16),
            pltpu.VMEM((pieces, rows, w), bf16),
            pltpu.VMEM((rows, 128), f32),
            pltpu.VMEM((n_fs, tokens, rows), bf16),
            pltpu.VMEM((tokens, w), f32),
            pltpu.VMEM((tokens, w), bf16),
            pltpu.VMEM((tokens, width), f32),
            dma((pieces,)), dma((2,)),
            dma((pieces,)), dma((pieces,)),
            dma((2, pieces)), dma((n_fs, n_c)),
            dma((n_fs, n_c)), dma((n_fs, n_c)),
            dma, dma,
            dma((n_c,)), dma((n_c,)),
            dma((n_c,)), dma((n_c,)),
        ] + (reduce_scratch if fused else []),
        compiler_params=pltpu.CompilerParams(collective_id=0, has_side_effects=True, vmem_limit_bytes=32000000),
    )(trained_up, trained_down, prompt_tokens[0], pre_gain[None], post_gain[None])
    if fused:
        return (result[None], sampler_up, sampler_down)

    layer_out = pl.pallas_call(
        functools.partial(sum_kernel, n_fs),
        out_shape=jax.ShapeDtypeStruct((share, width), bf16),
        in_specs=[vmem, vmem],
        out_specs=vmem,
        scratch_shapes=[pltpu.VMEM((n_fs, share, width), bf16), dma((n_fs - 1,)), dma((n_fs,))],
        compiler_params=pltpu.CompilerParams(collective_id=1, has_side_effects=True, vmem_limit_bytes=16000000),
    )(result.reshape(n_fs, share, width), post_gain[None])
    return (layer_out[None], sampler_up, sampler_down)


def solution(mesh):
    placed = (P("tp", None, None), P("fs", "tp"), P("fs", "tp"), P("fs"), P())
    return jax.shard_map(
        functools.partial(on_device, mesh.shape["fs"], mesh.shape["tp"]),
        mesh=mesh,
        in_specs=placed,
        out_specs=(P("tp", "fs", None), P(None, "fs"), P("fs", None)),
        check_vma=False,
    )
```

```python
import functools

import jax
import jax.numpy as jnp
from jax import lax
from jax.experimental import pallas as pl
from jax.experimental.pallas import tpu as pltpu
from jax.sharding import PartitionSpec as P

MESH = pl.DeviceIdType.MESH
EPS = 1e-06
CHUNK = 256
SEGMENTS = 4
GROUP = 4
PARTS = 4
DEPTH = 4


def remote(src, dst, send_sem, recv_sem, device):
    return pltpu.make_async_remote_copy(
        src_ref=src, dst_ref=dst, send_sem=send_sem, recv_sem=recv_sem, device_id=device, device_id_type=MESH
    )


def greet(device):
    pl.semaphore_signal(pltpu.get_barrier_semaphore(), inc=1, device_id=device, device_id_type=MESH)


def loop(count, body):
    lax.fori_loop(0, count, lambda i, c: (body(i), c)[1], 0)


def span(i, size):
    return pl.ds(pl.multiple_of(i * size, size), size)


def square_norm(values):
    return values * lax.rsqrt(jnp.mean(values * values, axis=-1, keepdims=True) + EPS)


def spread_kernel(
    n_fs, n_tp, w, fused,
    up_in, down_in, tokens, gain, post, held_up, held_down, out,
    stage, dstage, upb, xup, gcol, normed, acc, hid, pacc, us, ds_in,
    xs, xr, ps, pr, ws, wr, ns, nr, ds, dr, vs, vr, *reduce_refs,
):
    f, t = lax.axis_index("fs"), lax.axis_index("tp")
    far = lax.rem(t + n_tp // 2, n_tp)
    near = t + 1 - 2 * lax.rem(t, 2)
    near_far = lax.rem(near + n_tp // 2, n_tp)
    m = n_fs // n_tp
    rows, cols = up_in.shape
    owned = cols // m
    d_rows, d_width = down_in.shape
    width = n_tp * d_width
    n_c = owned // w
    d_part = d_rows // n_c
    pieces = m * n_c
    block_of_f = f // m
    active = lax.rem(lax.rem(block_of_f, 2) + lax.rem(t, 2), 2) == 0

    def load_up(k):
        return pltpu.make_async_copy(
            up_in.at[:, span(lax.rem(k, m) * n_c + k // m, w)], stage.at[k], us.at[k]
        )

    def load_down(c):
        return pltpu.make_async_copy(down_in.at[span(c, d_part)], dstage.at[lax.rem(c, 2)], ds_in.at[lax.rem(c, 2)])

    def landed(source, c):
        return held_up.at[span(source, rows), span(c, w)]

    n_s = PARTS if rows % (16 * PARTS) == 0 else 1
    sub = rows // n_s

    def x_copy(k, r):
        at = pl.ds(r * sub, sub)
        return remote(upb.at[k, at], xup.at[k, at], xs.at[k], xr.at[k, r], {"tp": far})

    def owner(phase, k):
        return (t if phase == 0 else far) * m + lax.rem(k, m)

    def peer_copy(phase, k, first, size):
        held = upb if phase == 0 else xup
        to = held_up.at[pl.ds(pl.multiple_of(f * rows + first, size), size), span(k // m, w)]
        return remote(
            held.at[k, pl.ds(first, size)], to, ps.at[phase, k], pr.at[f, k // m], {"fs": owner(phase, k)}
        )

    def start_peer(phase, k, r):
        @pl.when(owner(phase, k) != f)
        def _():
            peer_copy(phase, k, r * sub, sub).start()

    def end_peer(phase, k):
        @pl.when(owner(phase, k) != f)
        def _():
            peer_copy(phase, k, 0, rows).wait_send()

    def block(c, which):
        return held_down.at[span(c, d_part), span(which, d_width)]

    def d_copy(c):
        return remote(block(c, t), block(c, t), ds.at[c], dr.at[c], {"tp": far})

    def d_pass(c, which):
        return remote(block(c, which), block(c, which), vs.at[c], vr.at[c], {"tp": near})

    def column(which):
        return held_down.at[:, span(which, d_width)]

    def to_near(which):
        return remote(column(which), column(which), ns, nr, {"tp": near})

    def share(src, source, c):
        return remote(src, landed(source, c), ws.at[source, c], wr.at[source, c], {"tp": near})

    loop(n_fs - 1, lambda i: greet({"fs": lax.rem(f + 1 + i, n_fs)}))
    greet({"tp": far})
    greet({"tp": near})
    depth = min(DEPTH, pieces)
    loop(depth, lambda k: load_up(k).start())
    for c in range(min(2, n_c)):
        load_down(c).start()

    side = min(rows, 128)
    eye = lax.broadcasted_iota(jnp.int32, (side, side), 0) == lax.broadcasted_iota(jnp.int32, (side, side), 1)
    for b in range(rows // side):
        line = jnp.broadcast_to(gain[:, b * side : (b + 1) * side], (side, side))
        scale = jnp.sum(jnp.where(eye, line, 0.0), axis=1, keepdims=True)
        gcol[b * side : (b + 1) * side, :] = jnp.broadcast_to(scale, (side, 128))

    def convert(k):
        load_up(k).wait()

        @pl.when(k + depth < pieces)
        def _():
            load_up(k + depth).start()

        for j in range(0, w, 128):
            upb[k, :, j : j + 128] = (gcol[...] * stage[k, :, j : j + 128]).astype(upb.dtype)

    def send(k):
        for r in range(n_s):
            x_copy(k, r).start()
        for r in range(n_s):
            start_peer(0, k, r)

    convert(0)
    pl.semaphore_wait(pltpu.get_barrier_semaphore(), n_fs + 1)

    def convert_and_send(k):
        convert(k)
        send(k - 1)

    lax.fori_loop(1, pieces, lambda k, c: (convert_and_send(k), c)[1], 0)
    pacc[...] = jnp.zeros_like(pacc)
    send(pieces - 1)

    def convert_down(c):
        load_down(c).wait()
        held_down[span(c, d_part), span(t, d_width)] = dstage[lax.rem(c, 2)].astype(held_down.dtype)

        @pl.when(c + 2 < n_c)
        def _():
            load_down(c + 2).start()

    def pass_on(k):
        @pl.when(k == max(pieces - 2, 0))
        def _():
            loop(n_c, lambda c: d_copy(c).start())
            to_near(t).start()

        for r in range(n_s):
            x_copy(k, r).wait_recv()
            start_peer(1, k, r)

        @pl.when(k < n_c)
        def _():
            convert_down(k)

        @pl.when(k == n_c)
        def _():
            scaled = square_norm(tokens[...].astype(jnp.float32)).astype(jnp.bfloat16)
            for i in range(n_fs):
                normed[i] = scaled[:, i * rows : (i + 1) * rows]

    loop(pieces, pass_on)

    def gather(c):
        remote(block(c, far), block(c, far), ds.at[c], dr.at[c], {"tp": far}).wait_recv()
        d_pass(c, far).start()
        acc[...] = jnp.zeros_like(acc)

        def one(source):
            def keep_own(held):
                k = c * m + lax.rem(f, m)
                share(held.at[k], source, c).start()
                held_up[span(source, rows), span(c, w)] = held[k]

            @pl.when(jnp.logical_and(active, source == f))
            def _():
                @pl.when(block_of_f == t)
                def _():
                    keep_own(upb)

                @pl.when(block_of_f != t)
                def _():
                    keep_own(xup)

            @pl.when(jnp.logical_and(active, source != f))
            def _():
                remote(landed(source, c), landed(source, c), ws.at[source, c], pr.at[source, c], {"tp": near}).wait_recv()
                share(landed(source, c), source, c).start()

            @pl.when(jnp.logical_not(active))
            def _():
                share(landed(source, c), source, c).wait_recv()

            acc[...] += jnp.dot(
                normed[source], held_up[span(source, rows), span(c, w)], preferred_element_type=jnp.float32
            )

        loop(n_fs, one)
        hid[...] = jnp.square(jnp.maximum(acc[...], 0.0)).astype(jnp.bfloat16)
        d_pass(c, near_far).wait_recv()

        @pl.when(c == 0)
        def _():
            to_near(near).wait_recv()

    def add_down(c, first, count):
        tile = min(d_width, 512)

        def one(i):
            at = pl.ds(pl.multiple_of(first + i * tile, tile), tile)
            pacc[:, at] += jnp.dot(hid[...], held_down[span(c, d_part), at], preferred_element_type=jnp.float32)

        loop(count // tile, one)

    def whole_chunk(c):
        gather(c)
        add_down(c, 0, width)

    last = n_c - 1
    loop(last, whole_chunk)
    gather(last)
    if fused:
        sb, land, sb2, land2, fin, ss, rs, ss2, rs2 = reduce_refs
        _, q, n_o, part, seg = sb.shape
        i, o = lax.rem(f, q), f // q

        def peer(d):
            return lax.rem(i + d, q)

        def across(d):
            return lax.rem(o + d, n_o)

        def first_copy(s, d):
            return remote(sb.at[s, peer(d)], land.at[s, i], ss.at[s, d], rs.at[s, i], {"fs": o * q + peer(d)})

        def second_copy(s, d):
            return remote(sb2.at[s, across(d)], land2.at[s, o], ss2.at[s, d], rs2.at[s, o], {"fs": across(d) * q + i})

        for s in range(SEGMENTS):
            add_down(last, s * seg, seg)
            for b in range(n_o * q):
                sb[s, b % q, b // q] = pacc[b * part : (b + 1) * part, s * seg : (s + 1) * seg].astype(sb.dtype)
            for d in range(1, q):
                first_copy(s, d).start()

        for s in range(SEGMENTS):
            for d in range(1, q):
                remote(land.at[s, peer(d)], land.at[s, peer(d)], ss.at[s, d], rs.at[s, peer(d)], {"fs": f}).wait_recv()

            def total(to):
                value = pacc[span(to * q + i, part), s * seg : (s + 1) * seg]
                for d in range(1, q):
                    value += land[s, peer(d), to].astype(jnp.float32)
                return value

            for d in range(1, n_o):
                sb2[s, across(d)] = total(across(d)).astype(sb2.dtype)
            fin[:, s * seg : (s + 1) * seg] = total(o)
            for d in range(1, n_o):
                second_copy(s, d).start()

        for s in range(SEGMENTS):
            value = fin[:, s * seg : (s + 1) * seg]
            for d in range(1, n_o):
                remote(land2.at[s, across(d)], land2.at[s, across(d)], ss2.at[s, d], rs2.at[s, across(d)], {"fs": f}).wait_recv()
                value += land2[s, across(d)].astype(jnp.float32)
            fin[:, s * seg : (s + 1) * seg] = value
        total_sum = fin[...]
        scale = lax.rsqrt(jnp.mean(total_sum * total_sum, axis=-1, keepdims=True) + EPS)
        out[...] = (total_sum * scale * post[...]).astype(out.dtype)
        for s in range(SEGMENTS):
            for d in range(1, q):
                first_copy(s, d).wait_send()
            for d in range(1, n_o):
                second_copy(s, d).wait_send()
    else:
        add_down(last, 0, width)
        out[...] = pacc[...].astype(out.dtype)

    def ended(i):
        @pl.when(active)
        def _():
            source, c = i // n_c, lax.rem(i, n_c)
            share(landed(source, c), source, c).wait_send()

    loop(n_fs * n_c, ended)
    to_near(t).wait_send()

    def ended_down(c):
        d_copy(c).wait_send()
        d_pass(c, far).wait_send()

    loop(n_c, ended_down)

    def ended_pieces(k):
        remote(upb.at[k], xup.at[k], xs.at[k], xr.at[k, 0], {"tp": far}).wait_send()
        end_peer(0, k)
        end_peer(1, k)

    loop(pieces, ended_pieces)


def sum_kernel(n_fs, parts, gain, out, land, ss, rs):
    f = lax.axis_index("fs")

    def peer_of(i):
        return lax.rem(f + 1 + i, n_fs)

    loop(n_fs - 1, lambda i: greet({"fs": peer_of(i)}))
    pl.semaphore_wait(pltpu.get_barrier_semaphore(), n_fs - 1)

    def send(i):
        return remote(parts.at[peer_of(i)], land.at[f], ss.at[i], rs.at[f], {"fs": peer_of(i)})

    loop(n_fs - 1, lambda i: send(i).start())

    def add(i, total):
        source = peer_of(i)
        remote(land.at[source], land.at[source], ss.at[i], rs.at[source], {"fs": source}).wait_recv()
        return total + land[source].astype(jnp.float32)

    summed = lax.fori_loop(0, n_fs - 1, add, parts[f].astype(jnp.float32))
    scale = lax.rsqrt(jnp.mean(summed * summed, axis=-1, keepdims=True) + EPS)
    out[...] = (summed * scale * gain[...]).astype(out.dtype)
    loop(n_fs - 1, lambda i: send(i).wait_send())


def on_device(n_fs, n_tp, prompt_tokens, trained_up, trained_down, pre_gain, post_gain):
    bf16, f32 = jnp.bfloat16, jnp.float32
    rows, cols = trained_up.shape
    d_rows, d_cols = trained_down.shape
    tokens, width = prompt_tokens.shape[1:]
    m = n_fs // n_tp
    owned = cols // m
    w = min(owned, CHUNK)
    n_c = owned // w
    pieces = m * n_c
    share = tokens // n_fs
    q = GROUP
    n_o = n_fs // q
    seg = width // SEGMENTS
    fused = share % 16 == 0 and n_fs % q == 0 and n_o > 1
    anywhere = pl.BlockSpec(memory_space=pl.ANY)
    vmem = pl.BlockSpec(memory_space=pltpu.VMEM)
    dma = pltpu.SemaphoreType.DMA
    reduce_scratch = [
        pltpu.VMEM((SEGMENTS, q, n_o, share, seg), bf16),
        pltpu.VMEM((SEGMENTS, q, n_o, share, seg), bf16),
        pltpu.VMEM((SEGMENTS, n_o, share, seg), bf16),
        pltpu.VMEM((SEGMENTS, n_o, share, seg), bf16),
        pltpu.VMEM((share, width), f32),
        dma((SEGMENTS, q)), dma((SEGMENTS, q)),
        dma((SEGMENTS, n_o)), dma((SEGMENTS, n_o)),
    ]
    sampler_up, sampler_down, result = pl.pallas_call(
        functools.partial(spread_kernel, n_fs, n_tp, w, fused),
        out_shape=(
            pltpu.VMEM((n_fs * rows, owned), bf16),
            pltpu.VMEM((d_rows, n_tp * d_cols), bf16),
            jax.ShapeDtypeStruct((share if fused else tokens, width), bf16),
        ),
        in_specs=[anywhere, anywhere, vmem, vmem, vmem],
        out_specs=(vmem, vmem, vmem),
        scratch_shapes=[
            pltpu.VMEM((pieces, rows, w), f32),
            pltpu.VMEM((2, d_rows // n_c, d_cols), f32),
            pltpu.VMEM((pieces, rows, w), bf16),
            pltpu.VMEM((pieces, rows, w), bf16),
            pltpu.VMEM((rows, 128), f32),
            pltpu.VMEM((n_fs, tokens, rows), bf16),
            pltpu.VMEM((tokens, w), f32),
            pltpu.VMEM((tokens, w), bf16),
            pltpu.VMEM((tokens, width), f32),
            dma((pieces,)), dma((2,)),
            dma((pieces,)), dma((pieces, PARTS)),
            dma((2, pieces)), dma((n_fs, n_c)),
            dma((n_fs, n_c)), dma((n_fs, n_c)),
            dma, dma,
            dma((n_c,)), dma((n_c,)),
            dma((n_c,)), dma((n_c,)),
        ] + (reduce_scratch if fused else []),
        compiler_params=pltpu.CompilerParams(collective_id=0, has_side_effects=True, vmem_limit_bytes=32000000),
    )(trained_up, trained_down, prompt_tokens[0], pre_gain[None], post_gain[None])
    if fused:
        return (result[None], sampler_up, sampler_down)

    layer_out = pl.pallas_call(
        functools.partial(sum_kernel, n_fs),
        out_shape=jax.ShapeDtypeStruct((share, width), bf16),
        in_specs=[vmem, vmem],
        out_specs=vmem,
        scratch_shapes=[pltpu.VMEM((n_fs, share, width), bf16), dma((n_fs - 1,)), dma((n_fs,))],
        compiler_params=pltpu.CompilerParams(collective_id=1, has_side_effects=True, vmem_limit_bytes=16000000),
    )(result.reshape(n_fs, share, width), post_gain[None])
    return (layer_out[None], sampler_up, sampler_down)


def solution(mesh):
    placed = (P("tp", None, None), P("fs", "tp"), P("fs", "tp"), P("fs"), P())
    return jax.shard_map(
        functools.partial(on_device, mesh.shape["fs"], mesh.shape["tp"]),
        mesh=mesh,
        in_specs=placed,
        out_specs=(P("tp", "fs", None), P(None, "fs"), P("fs", None)),
        check_vma=False,
    )
```

```python
import functools

import jax
import jax.numpy as jnp
from jax import lax
from jax.experimental import pallas as pl
from jax.experimental.pallas import tpu as pltpu
from jax.sharding import PartitionSpec as P

MESH = pl.DeviceIdType.MESH
EPS = 1e-06
CHUNK = 256
SEGMENTS = 4
GROUP = 4
STORES = 4
PARTS = 4
DEPTH = 4


def remote(src, dst, send_sem, recv_sem, device):
    return pltpu.make_async_remote_copy(
        src_ref=src, dst_ref=dst, send_sem=send_sem, recv_sem=recv_sem, device_id=device, device_id_type=MESH
    )


def greet(device):
    pl.semaphore_signal(pltpu.get_barrier_semaphore(), inc=1, device_id=device, device_id_type=MESH)


def loop(count, body):
    lax.fori_loop(0, count, lambda i, c: (body(i), c)[1], 0)


def span(i, size):
    return pl.ds(pl.multiple_of(i * size, size), size)


def square_norm(values):
    return values * lax.rsqrt(jnp.mean(values * values, axis=-1, keepdims=True) + EPS)


def spread_kernel(
    n_fs, n_tp, w, fused,
    up_in, down_in, tokens, gain, post, held_up, held_down, pacc, out,
    stage, dstage, upb, xup, gcol, normed, acc, hid, us, ds_in,
    xs, xr, ps, pr, ws, wr, ns, nr, ds, dr, vs, vr, *reduce_refs,
):
    f, t = lax.axis_index("fs"), lax.axis_index("tp")
    far = lax.rem(t + n_tp // 2, n_tp)
    near = t + 1 - 2 * lax.rem(t, 2)
    near_far = lax.rem(near + n_tp // 2, n_tp)
    m = n_fs // n_tp
    rows, cols = up_in.shape
    owned = cols // m
    d_rows, d_width = down_in.shape
    width = n_tp * d_width
    n_c = owned // w
    d_part = d_rows // n_c
    pieces = m * n_c
    block_of_f = f // m
    active = lax.rem(lax.rem(block_of_f, 2) + lax.rem(t, 2), 2) == 0

    def load_up(k):
        return pltpu.make_async_copy(
            up_in.at[:, span(lax.rem(k, m) * n_c + k // m, w)], stage.at[k], us.at[k]
        )

    def load_down(c):
        return pltpu.make_async_copy(down_in.at[span(c, d_part)], dstage.at[lax.rem(c, 2)], ds_in.at[lax.rem(c, 2)])

    def landed(source, c):
        return held_up.at[span(source, rows), span(c, w)]

    n_s = PARTS if rows % (16 * PARTS) == 0 else 1
    sub = rows // n_s

    def x_copy(k, r):
        at = pl.ds(r * sub, sub)
        return remote(upb.at[k, at], xup.at[k, at], xs.at[k], xr.at[k, r], {"tp": far})

    def owner(phase, k):
        return (t if phase == 0 else far) * m + lax.rem(k, m)

    def peer_copy(phase, k, first, size):
        held = upb if phase == 0 else xup
        to = held_up.at[pl.ds(pl.multiple_of(f * rows + first, size), size), span(k // m, w)]
        return remote(
            held.at[k, pl.ds(first, size)], to, ps.at[phase, k], pr.at[f, k // m], {"fs": owner(phase, k)}
        )

    def start_peer(phase, k, r):
        @pl.when(owner(phase, k) != f)
        def _():
            peer_copy(phase, k, r * sub, sub).start()

    def end_peer(phase, k):
        @pl.when(owner(phase, k) != f)
        def _():
            peer_copy(phase, k, 0, rows).wait_send()

    def block(c, which):
        return held_down.at[span(c, d_part), span(which, d_width)]

    def d_copy(c):
        return remote(block(c, t), block(c, t), ds.at[c], dr.at[c], {"tp": far})

    def d_pass(c, which):
        return remote(block(c, which), block(c, which), vs.at[c], vr.at[c], {"tp": near})

    def column(which):
        return held_down.at[:, span(which, d_width)]

    def to_near(which):
        return remote(column(which), column(which), ns, nr, {"tp": near})

    def share(src, source, c):
        return remote(src, landed(source, c), ws.at[source, c], wr.at[source, c], {"tp": near})

    loop(n_fs - 1, lambda i: greet({"fs": lax.rem(f + 1 + i, n_fs)}))
    greet({"tp": far})
    greet({"tp": near})
    depth = min(DEPTH, pieces)
    loop(depth, lambda k: load_up(k).start())
    for c in range(min(2, n_c)):
        load_down(c).start()

    side = min(rows, 128)
    eye = lax.broadcasted_iota(jnp.int32, (side, side), 0) == lax.broadcasted_iota(jnp.int32, (side, side), 1)
    for b in range(rows // side):
        line = jnp.broadcast_to(gain[:, b * side : (b + 1) * side], (side, side))
        scale = jnp.sum(jnp.where(eye, line, 0.0), axis=1, keepdims=True)
        gcol[b * side : (b + 1) * side, :] = jnp.broadcast_to(scale, (side, 128))

    def convert(k):
        load_up(k).wait()

        @pl.when(k + depth < pieces)
        def _():
            load_up(k + depth).start()

        for j in range(0, w, 128):
            upb[k, :, j : j + 128] = (gcol[...] * stage[k, :, j : j + 128]).astype(upb.dtype)

    def send(k):
        for r in range(n_s):
            x_copy(k, r).start()
        for r in range(n_s):
            start_peer(0, k, r)

    convert(0)
    pl.semaphore_wait(pltpu.get_barrier_semaphore(), n_fs + 1)

    def convert_and_send(k):
        convert(k)
        send(k - 1)

    lax.fori_loop(1, pieces, lambda k, c: (convert_and_send(k), c)[1], 0)
    pacc[...] = jnp.zeros_like(pacc)
    send(pieces - 1)

    def convert_down(c):
        load_down(c).wait()
        held_down[span(c, d_part), span(t, d_width)] = dstage[lax.rem(c, 2)].astype(held_down.dtype)

        @pl.when(c + 2 < n_c)
        def _():
            load_down(c + 2).start()

    def pass_on(k):
        @pl.when(k == max(pieces - 2, 0))
        def _():
            loop(n_c, lambda c: d_copy(c).start())
            to_near(t).start()

        for r in range(n_s):
            x_copy(k, r).wait_recv()
            start_peer(1, k, r)

        @pl.when(k < n_c)
        def _():
            convert_down(k)

        @pl.when(k == n_c)
        def _():
            scaled = square_norm(tokens[...].astype(jnp.float32)).astype(jnp.bfloat16)
            for i in range(n_fs):
                normed[i] = scaled[:, i * rows : (i + 1) * rows]

    loop(pieces, pass_on)

    def gather(c):
        remote(block(c, far), block(c, far), ds.at[c], dr.at[c], {"tp": far}).wait_recv()
        d_pass(c, far).start()
        acc[...] = jnp.zeros_like(acc)

        def one(step):
            half = n_fs // 2
            side = lax.rem(f // half + step // half, 2)
            source = side * half + lax.rem(f + step, half)

            def keep_own(held):
                k = c * m + lax.rem(f, m)
                share(held.at[k], source, c).start()
                held_up[span(source, rows), span(c, w)] = held[k]

            @pl.when(jnp.logical_and(active, source == f))
            def _():
                @pl.when(block_of_f == t)
                def _():
                    keep_own(upb)

                @pl.when(block_of_f != t)
                def _():
                    keep_own(xup)

            @pl.when(jnp.logical_and(active, source != f))
            def _():
                remote(landed(source, c), landed(source, c), ws.at[source, c], pr.at[source, c], {"tp": near}).wait_recv()
                share(landed(source, c), source, c).start()

            @pl.when(jnp.logical_not(active))
            def _():
                share(landed(source, c), source, c).wait_recv()

            acc[...] += jnp.dot(
                normed[source], held_up[span(source, rows), span(c, w)], preferred_element_type=jnp.float32
            )

        loop(n_fs, one)
        hid[...] = jnp.square(jnp.maximum(acc[...], 0.0)).astype(jnp.bfloat16)
        d_pass(c, near_far).wait_recv()

        @pl.when(c == 0)
        def _():
            to_near(near).wait_recv()

    def add_down(c, first, count):
        tile = min(d_width, 512)

        def one(i):
            at = pl.ds(pl.multiple_of(first + i * tile, tile), tile)
            pacc[:, at] += jnp.dot(hid[...], held_down[span(c, d_part), at], preferred_element_type=jnp.float32)

        loop(count // tile, one)

    def whole_chunk(c):
        gather(c)
        add_down(c, 0, width)

    last = n_c - 1
    loop(last, whole_chunk)
    gather(last)
    if fused:
        @pl.when(lax.rem(t, 2) == 0)
        def _():
            reduce_rows(pacc, post, out, lambda s, seg: add_down(last, s * seg, seg), *reduce_refs)

        @pl.when(lax.rem(t, 2) == 1)
        def _():
            add_down(last, 0, width)
    else:
        add_down(last, 0, width)
        out[...] = jnp.zeros_like(out)

    def ended(i):
        @pl.when(active)
        def _():
            source, c = i // n_c, lax.rem(i, n_c)
            share(landed(source, c), source, c).wait_send()

    loop(n_fs * n_c, ended)
    to_near(t).wait_send()

    def ended_down(c):
        d_copy(c).wait_send()
        d_pass(c, far).wait_send()

    loop(n_c, ended_down)

    def ended_pieces(k):
        remote(upb.at[k], xup.at[k], xs.at[k], xr.at[k, 0], {"tp": far}).wait_send()
        end_peer(0, k)
        end_peer(1, k)

    loop(pieces, ended_pieces)


def reduce_rows(pacc, post, out, compute, sb, land, sb2, land2, fin, ss, rs, ss2, rs2):
    f = lax.axis_index("fs")
    _, q, n_o, part, seg = sb.shape
    i, o = lax.rem(f, q), f // q

    def peer(d):
        return lax.rem(i + d, q)

    def across(d):
        return lax.rem(o + d, n_o)

    def first_copy(s, d):
        return remote(sb.at[s, peer(d)], land.at[s, i], ss.at[s, d], rs.at[s, i], {"fs": o * q + peer(d)})

    def second_copy(s, d):
        return remote(sb2.at[s, across(d)], land2.at[s, o], ss2.at[s, d], rs2.at[s, o], {"fs": across(d) * q + i})

    def fill(s):
        for b in range(n_o * q):
            sb[s, b % q, b // q] = pacc[b * part : (b + 1) * part, s * seg : (s + 1) * seg].astype(sb.dtype)

    def send(s):
        for d in range(1, q):
            first_copy(s, d).start()

    if compute is None:
        for s in range(SEGMENTS):
            fill(s)
        pl.semaphore_wait(pltpu.get_barrier_semaphore(), n_o * q - 1)
        for s in range(SEGMENTS):
            send(s)
    else:
        for s in range(SEGMENTS):
            compute(s, seg)
            fill(s)
            send(s)

    for s in range(SEGMENTS):
        for d in range(1, q):
            remote(land.at[s, peer(d)], land.at[s, peer(d)], ss.at[s, d], rs.at[s, peer(d)], {"fs": f}).wait_recv()

        def total(to):
            value = pacc[span(to * q + i, part), s * seg : (s + 1) * seg]
            for d in range(1, q):
                value += land[s, peer(d), to].astype(jnp.float32)
            return value

        for d in range(1, n_o):
            sb2[s, across(d)] = total(across(d)).astype(sb2.dtype)
        fin[:, s * seg : (s + 1) * seg] = total(o)
        for d in range(1, n_o):
            second_copy(s, d).start()

    for s in range(SEGMENTS):
        value = fin[:, s * seg : (s + 1) * seg]
        for d in range(1, n_o):
            remote(land2.at[s, across(d)], land2.at[s, across(d)], ss2.at[s, d], rs2.at[s, across(d)], {"fs": f}).wait_recv()
            value += land2[s, across(d)].astype(jnp.float32)
        fin[:, s * seg : (s + 1) * seg] = value
    summed = fin[...]
    scale = lax.rsqrt(jnp.mean(summed * summed, axis=-1, keepdims=True) + EPS)
    out[...] = (summed * scale * post[...]).astype(out.dtype)
    for s in range(SEGMENTS):
        for d in range(1, q):
            first_copy(s, d).wait_send()
        for d in range(1, n_o):
            second_copy(s, d).wait_send()


def late_kernel(n_fs, pacc, post, early, up_token, down_token, out, *refs):
    f, t = lax.axis_index("fs"), lax.axis_index("tp")

    @pl.when(lax.rem(t, 2) == 1)
    def _():
        loop(n_fs - 1, lambda i: greet({"fs": lax.rem(f + 1 + i, n_fs)}))
        reduce_rows(pacc, post, out, None, *refs)

    @pl.when(lax.rem(t, 2) == 0)
    def _():
        out[...] = early[...]


def store_kernel(src, dst, token, sems):
    count = sems.shape[0]
    size = src.shape[0] // count
    copies = [
        pltpu.make_async_copy(src.at[pl.ds(p * size, size)], dst.at[pl.ds(p * size, size)], sems.at[p])
        for p in range(count)
    ]
    for copy in copies:
        copy.start()
    token[...] = jnp.zeros_like(token)
    for copy in copies:
        copy.wait()


def store(array):
    return pl.pallas_call(
        store_kernel,
        out_shape=(jax.ShapeDtypeStruct(array.shape, array.dtype), jax.ShapeDtypeStruct((8, 128), jnp.float32)),
        in_specs=[pl.BlockSpec(memory_space=pltpu.VMEM)],
        out_specs=(pl.BlockSpec(memory_space=pl.ANY), pl.BlockSpec(memory_space=pltpu.VMEM)),
        scratch_shapes=[pltpu.SemaphoreType.DMA((STORES,))],
        compiler_params=pltpu.CompilerParams(vmem_limit_bytes=1000000),
    )(array)


def sum_kernel(n_fs, parts, gain, out, land, ss, rs):
    f = lax.axis_index("fs")

    def peer_of(i):
        return lax.rem(f + 1 + i, n_fs)

    loop(n_fs - 1, lambda i: greet({"fs": peer_of(i)}))
    pl.semaphore_wait(pltpu.get_barrier_semaphore(), n_fs - 1)

    def send(i):
        return remote(parts.at[peer_of(i)], land.at[f], ss.at[i], rs.at[f], {"fs": peer_of(i)})

    loop(n_fs - 1, lambda i: send(i).start())

    def add(i, total):
        source = peer_of(i)
        remote(land.at[source], land.at[source], ss.at[i], rs.at[source], {"fs": source}).wait_recv()
        return total + land[source].astype(jnp.float32)

    summed = lax.fori_loop(0, n_fs - 1, add, parts[f].astype(jnp.float32))
    scale = lax.rsqrt(jnp.mean(summed * summed, axis=-1, keepdims=True) + EPS)
    out[...] = (summed * scale * gain[...]).astype(out.dtype)
    loop(n_fs - 1, lambda i: send(i).wait_send())


def on_device(n_fs, n_tp, prompt_tokens, trained_up, trained_down, pre_gain, post_gain):
    bf16, f32 = jnp.bfloat16, jnp.float32
    rows, cols = trained_up.shape
    d_rows, d_cols = trained_down.shape
    tokens, width = prompt_tokens.shape[1:]
    m = n_fs // n_tp
    owned = cols // m
    w = min(owned, CHUNK)
    n_c = owned // w
    pieces = m * n_c
    share = tokens // n_fs
    q = GROUP
    n_o = n_fs // q
    seg = width // SEGMENTS
    fused = share % 16 == 0 and n_fs % q == 0 and n_o > 1
    anywhere = pl.BlockSpec(memory_space=pl.ANY)
    vmem = pl.BlockSpec(memory_space=pltpu.VMEM)
    dma = pltpu.SemaphoreType.DMA
    reduce_scratch = [
        pltpu.VMEM((SEGMENTS, q, n_o, share, seg), bf16),
        pltpu.VMEM((SEGMENTS, q, n_o, share, seg), bf16),
        pltpu.VMEM((SEGMENTS, n_o, share, seg), bf16),
        pltpu.VMEM((SEGMENTS, n_o, share, seg), bf16),
        pltpu.VMEM((share, width), f32),
        dma((SEGMENTS, q)), dma((SEGMENTS, q)),
        dma((SEGMENTS, n_o)), dma((SEGMENTS, n_o)),
    ]
    held_up, held_down, parts, early = pl.pallas_call(
        functools.partial(spread_kernel, n_fs, n_tp, w, fused),
        out_shape=(
            pltpu.VMEM((n_fs * rows, owned), bf16),
            pltpu.VMEM((d_rows, n_tp * d_cols), bf16),
            pltpu.VMEM((tokens, width), f32),
            jax.ShapeDtypeStruct((share, width), bf16),
        ),
        in_specs=[anywhere, anywhere, vmem, vmem, vmem],
        out_specs=(vmem, vmem, vmem, vmem),
        scratch_shapes=[
            pltpu.VMEM((pieces, rows, w), f32),
            pltpu.VMEM((2, d_rows // n_c, d_cols), f32),
            pltpu.VMEM((pieces, rows, w), bf16),
            pltpu.VMEM((pieces, rows, w), bf16),
            pltpu.VMEM((rows, 128), f32),
            pltpu.VMEM((n_fs, tokens, rows), bf16),
            pltpu.VMEM((tokens, w), f32),
            pltpu.VMEM((tokens, w), bf16),
            dma((pieces,)), dma((2,)),
            dma((pieces,)), dma((pieces, PARTS)),
            dma((2, pieces)), dma((n_fs, n_c)),
            dma((n_fs, n_c)), dma((n_fs, n_c)),
            dma, dma,
            dma((n_c,)), dma((n_c,)),
            dma((n_c,)), dma((n_c,)),
        ] + (reduce_scratch if fused else []),
        compiler_params=pltpu.CompilerParams(collective_id=0, has_side_effects=True, vmem_limit_bytes=30500000),
    )(trained_up, trained_down, prompt_tokens[0], pre_gain[None], post_gain[None])
    sampler_up, up_token = store(held_up)
    sampler_down, down_token = store(held_down)
    if fused:
        layer_out = pl.pallas_call(
            functools.partial(late_kernel, n_fs),
            out_shape=jax.ShapeDtypeStruct((share, width), bf16),
            in_specs=[vmem, vmem, vmem, anywhere, anywhere],
            out_specs=vmem,
            scratch_shapes=reduce_scratch,
            compiler_params=pltpu.CompilerParams(collective_id=1, has_side_effects=True, vmem_limit_bytes=16000000),
        )(parts, post_gain[None], early, up_token, down_token)
        return (layer_out[None], sampler_up, sampler_down)

    layer_out = pl.pallas_call(
        functools.partial(sum_kernel, n_fs),
        out_shape=jax.ShapeDtypeStruct((share, width), bf16),
        in_specs=[vmem, vmem],
        out_specs=vmem,
        scratch_shapes=[pltpu.VMEM((n_fs, share, width), bf16), dma((n_fs - 1,)), dma((n_fs,))],
        compiler_params=pltpu.CompilerParams(collective_id=1, has_side_effects=True, vmem_limit_bytes=16000000),
    )(parts.astype(bf16).reshape(n_fs, share, width), post_gain[None])
    return (layer_out[None], sampler_up, sampler_down)


def solution(mesh):
    placed = (P("tp", None, None), P("fs", "tp"), P("fs", "tp"), P("fs"), P())
    return jax.shard_map(
        functools.partial(on_device, mesh.shape["fs"], mesh.shape["tp"]),
        mesh=mesh,
        in_specs=placed,
        out_specs=(P("tp", "fs", None), P(None, "fs"), P("fs", None)),
        check_vma=False,
    )
```

```python
import functools

import jax
import jax.numpy as jnp
from jax import lax
from jax.experimental import pallas as pl
from jax.experimental.pallas import tpu as pltpu
from jax.sharding import PartitionSpec as P

MESH = pl.DeviceIdType.MESH
EPS = 1e-06
CHUNK = 256
SEGMENTS = 4
GROUP = 4
STORES = 4
PARTS = 4
DEPTH = 4


def remote(src, dst, send_sem, recv_sem, device):
    return pltpu.make_async_remote_copy(
        src_ref=src, dst_ref=dst, send_sem=send_sem, recv_sem=recv_sem, device_id=device, device_id_type=MESH
    )


def greet(device):
    pl.semaphore_signal(pltpu.get_barrier_semaphore(), inc=1, device_id=device, device_id_type=MESH)


def loop(count, body):
    lax.fori_loop(0, count, lambda i, c: (body(i), c)[1], 0)


def span(i, size):
    return pl.ds(pl.multiple_of(i * size, size), size)


def square_norm(values):
    return values * lax.rsqrt(jnp.mean(values * values, axis=-1, keepdims=True) + EPS)


def spread_kernel(
    n_fs, n_tp, w, fused,
    up_in, down_in, tokens, gain, post, held_up, held_down, pacc, hid, out,
    stage, dstage, upb, xup, gcol, normed, acc, us, ds_in,
    xs, xr, ps, pr, ws, wr, ns, nr, ds, dr, vs, vr, *reduce_refs,
):
    f, t = lax.axis_index("fs"), lax.axis_index("tp")
    far = lax.rem(t + n_tp // 2, n_tp)
    near = t + 1 - 2 * lax.rem(t, 2)
    near_far = lax.rem(near + n_tp // 2, n_tp)
    m = n_fs // n_tp
    rows, cols = up_in.shape
    owned = cols // m
    d_rows, d_width = down_in.shape
    width = n_tp * d_width
    n_c = owned // w
    d_part = d_rows // n_c
    pieces = m * n_c
    block_of_f = f // m
    active = lax.rem(lax.rem(block_of_f, 2) + lax.rem(t, 2), 2) == 0

    depth = stage.shape[0]

    def load_up(k):
        return pltpu.make_async_copy(
            up_in.at[:, span(lax.rem(k, m) * n_c + k // m, w)], stage.at[lax.rem(k, depth)], us.at[lax.rem(k, depth)]
        )

    def load_down(c):
        return pltpu.make_async_copy(down_in.at[span(c, d_part)], dstage.at[lax.rem(c, 2)], ds_in.at[lax.rem(c, 2)])

    def landed(source, c):
        return held_up.at[span(source, rows), span(c, w)]

    n_s = PARTS if rows % (16 * PARTS) == 0 else 1
    sub = rows // n_s

    def x_part(k, r):
        at = pl.ds(r * sub, sub)
        return remote(upb.at[k, at], xup.at[k, at], xs, xr.at[k * n_s + r], {"tp": far})

    def x_copy(k):
        return remote(upb.at[k], xup.at[k], xs, xr.at[m * (n_s - 1) + k], {"tp": far})

    def owner(phase, k):
        return (t if phase == 0 else far) * m + lax.rem(k, m)

    def peer_copy(phase, k, first, size):
        held = upb if phase == 0 else xup
        to = held_up.at[pl.ds(pl.multiple_of(f * rows + first, size), size), span(k // m, w)]
        return remote(
            held.at[k, pl.ds(first, size)], to, ps.at[phase], pr.at[f, k // m], {"fs": owner(phase, k)}
        )

    def start_peer(phase, k, first, size):
        @pl.when(owner(phase, k) != f)
        def _():
            peer_copy(phase, k, first, size).start()

    def end_peers(phase):
        held = upb if phase == 0 else xup
        own = block_of_f == (t if phase == 0 else far)

        def ended(count):
            sent = held.at[pl.ds(0, count)]
            remote(sent, sent, ps.at[phase], ps.at[phase], {"tp": far}).wait_send()

        @pl.when(own)
        def _():
            ended(pieces - n_c)

        @pl.when(jnp.logical_not(own))
        def _():
            ended(pieces)

    def block(c, which):
        return held_down.at[span(c, d_part), span(which, d_width)]

    def d_copy(c):
        return remote(block(c, t), block(c, t), ds, dr.at[c], {"tp": far})

    def d_pass(c, which):
        return remote(block(c, which), block(c, which), vs, vr.at[c], {"tp": near})

    def column(which):
        return held_down.at[:, span(which, d_width)]

    def to_near(which):
        return remote(column(which), column(which), ns, nr, {"tp": near})

    def share(src, source, c):
        return remote(src, landed(source, c), ws, wr.at[source, c], {"tp": near})

    loop(n_fs - 1, lambda i: greet({"fs": lax.rem(f + 1 + i, n_fs)}))
    greet({"tp": far})
    greet({"tp": near})
    loop(depth, lambda k: load_up(k).start())
    for c in range(min(2, n_c)):
        load_down(c).start()

    side = min(rows, 128)
    eye = lax.broadcasted_iota(jnp.int32, (side, side), 0) == lax.broadcasted_iota(jnp.int32, (side, side), 1)
    for b in range(rows // side):
        line = jnp.broadcast_to(gain[:, b * side : (b + 1) * side], (side, side))
        scale = jnp.sum(jnp.where(eye, line, 0.0), axis=1, keepdims=True)
        gcol[b * side : (b + 1) * side, :] = jnp.broadcast_to(scale, (side, 128))

    def convert(k):
        load_up(k).wait()
        for j in range(0, w, 128):
            upb[k, :, j : j + 128] = (gcol[...] * stage[lax.rem(k, depth), :, j : j + 128]).astype(upb.dtype)

        @pl.when(k + depth < pieces)
        def _():
            load_up(k + depth).start()

    def send_parts(k):
        for r in range(n_s):
            x_part(k, r).start()
        for r in range(n_s):
            start_peer(0, k, r * sub, sub)

    def send(k):
        x_copy(k).start()
        start_peer(0, k, 0, rows)

    convert(0)
    pl.semaphore_wait(pltpu.get_barrier_semaphore(), n_fs + 1)

    for k in range(min(m, pieces - 1)):
        convert(k + 1)
        send_parts(k)

    def convert_and_send(k):
        convert(k)
        send(k - 1)

    lax.fori_loop(m + 1, pieces, lambda k, c: (convert_and_send(k), c)[1], 0)
    pacc[...] = jnp.zeros_like(pacc)
    (send if pieces > m else send_parts)(pieces - 1)

    def convert_down(c):
        load_down(c).wait()
        held_down[span(c, d_part), span(t, d_width)] = dstage[lax.rem(c, 2)].astype(held_down.dtype)

        @pl.when(c + 2 < n_c)
        def _():
            load_down(c + 2).start()

    def between(k):
        @pl.when(k == max(pieces - 2, 0))
        def _():
            loop(n_c, lambda c: d_copy(c).start())
            to_near(t).start()

        @pl.when(k < n_c)
        def _():
            convert_down(k)

        @pl.when(k == n_c)
        def _():
            scaled = square_norm(tokens[...].astype(jnp.float32)).astype(jnp.bfloat16)
            for i in range(n_fs):
                normed[i] = scaled[:, i * rows : (i + 1) * rows]

    def pass_parts(k):
        for r in range(n_s):
            x_part(k, r).wait_recv()
            start_peer(1, k, r * sub, sub)
        between(k)

    def pass_on(k):
        x_copy(k).wait_recv()
        start_peer(1, k, 0, rows)
        between(k)

    loop(m, pass_parts)
    lax.fori_loop(m, pieces, lambda k, c: (pass_on(k), c)[1], 0)

    def gather(c):
        remote(block(c, far), block(c, far), ds, dr.at[c], {"tp": far}).wait_recv()
        d_pass(c, far).start()
        acc[...] = jnp.zeros_like(acc)

        def one(step):
            half = n_fs // 2
            side = lax.rem(f // half + step // half, 2)
            source = side * half + lax.rem(f + step, half)

            def keep_own(held):
                k = c * m + lax.rem(f, m)
                share(held.at[k], source, c).start()
                held_up[span(source, rows), span(c, w)] = held[k]

            @pl.when(jnp.logical_and(active, source == f))
            def _():
                @pl.when(block_of_f == t)
                def _():
                    keep_own(upb)

                @pl.when(block_of_f != t)
                def _():
                    keep_own(xup)

            @pl.when(jnp.logical_and(active, source != f))
            def _():
                remote(landed(source, c), landed(source, c), ws, pr.at[source, c], {"tp": near}).wait_recv()
                share(landed(source, c), source, c).start()

            @pl.when(jnp.logical_not(active))
            def _():
                share(landed(source, c), source, c).wait_recv()

            acc[...] += jnp.dot(
                normed[source], held_up[span(source, rows), span(c, w)], preferred_element_type=jnp.float32
            )

        loop(n_fs, one)
        hid[...] = jnp.square(jnp.maximum(acc[...], 0.0)).astype(jnp.bfloat16)
        d_pass(c, near_far).wait_recv()

        @pl.when(c == 0)
        def _():
            to_near(near).wait_recv()

    def add_down(c, first, count):
        tile = min(d_width, 512)

        def one(i):
            at = pl.ds(pl.multiple_of(first + i * tile, tile), tile)
            pacc[:, at] += jnp.dot(hid[...], held_down[span(c, d_part), at], preferred_element_type=jnp.float32)

        loop(count // tile, one)

    def whole_chunk(c):
        gather(c)
        add_down(c, 0, width)

    last = n_c - 1
    loop(last, whole_chunk)
    gather(last)
    if fused:
        @pl.when(lax.rem(t, 2) == 0)
        def _():
            reduce_rows(pacc, post, out, lambda s, seg: add_down(last, s * seg, seg), False, *reduce_refs)
    else:
        add_down(last, 0, width)
        out[...] = jnp.zeros_like(out)

    @pl.when(active)
    def _():
        remote(held_up, held_up, ws, ws, {"tp": near}).wait_send()

    to_near(t).wait_send()
    remote(column(t), column(t), ds, ds, {"tp": far}).wait_send()
    remote(column(far), column(far), vs, vs, {"tp": near}).wait_send()
    remote(upb, xup, xs, xs, {"tp": far}).wait_send()
    end_peers(0)
    end_peers(1)


def reduce_rows(pacc, post, out, compute, waiting, sb, land, sb2, land2, fin, ss, rs, ss2, rs2):
    f = lax.axis_index("fs")
    _, q, n_o, part, seg = sb.shape
    i, o = lax.rem(f, q), f // q

    def peer(d):
        return lax.rem(i + d, q)

    def across(d):
        return lax.rem(o + d, n_o)

    def first_copy(s, d):
        return remote(sb.at[s, peer(d)], land.at[s, i], ss, rs.at[s, i], {"fs": o * q + peer(d)})

    def second_copy(s, d):
        return remote(sb2.at[s, across(d)], land2.at[s, o], ss2, rs2.at[s, o], {"fs": across(d) * q + i})

    def fill(s):
        for b in range(n_o * q):
            sb[s, b % q, b // q] = pacc[b * part : (b + 1) * part, s * seg : (s + 1) * seg].astype(sb.dtype)

    def send(s):
        for d in range(1, q):
            first_copy(s, d).start()

    if waiting:
        for s in range(SEGMENTS):
            compute(s, seg)
            fill(s)
        pl.semaphore_wait(pltpu.get_barrier_semaphore(), n_o * q - 1)
        for s in range(SEGMENTS):
            send(s)
    else:
        for s in range(SEGMENTS):
            compute(s, seg)
            fill(s)
            send(s)

    for s in range(SEGMENTS):
        for d in range(1, q):
            remote(land.at[s, peer(d)], land.at[s, peer(d)], ss, rs.at[s, peer(d)], {"fs": f}).wait_recv()

        def total(to):
            value = pacc[span(to * q + i, part), s * seg : (s + 1) * seg]
            for d in range(1, q):
                value += land[s, peer(d), to].astype(jnp.float32)
            return value

        for d in range(1, n_o):
            sb2[s, across(d)] = total(across(d)).astype(sb2.dtype)
        fin[:, s * seg : (s + 1) * seg] = total(o)
        for d in range(1, n_o):
            second_copy(s, d).start()

    for s in range(SEGMENTS):
        value = fin[:, s * seg : (s + 1) * seg]
        for d in range(1, n_o):
            remote(land2.at[s, across(d)], land2.at[s, across(d)], ss2, rs2.at[s, across(d)], {"fs": f}).wait_recv()
            value += land2[s, across(d)].astype(jnp.float32)
        fin[:, s * seg : (s + 1) * seg] = value
    summed = fin[...]
    scale = lax.rsqrt(jnp.mean(summed * summed, axis=-1, keepdims=True) + EPS)
    out[...] = (summed * scale * post[...]).astype(out.dtype)
    for buffer, count, sem in ((sb, q - 1, ss), (sb2, n_o - 1, ss2)):
        sent = buffer.at[:, pl.ds(0, count)]
        remote(sent, sent, sem, sem, {"fs": f}).wait_send()


def late_kernel(n_fs, parts, hidden, held_down, post, early, up_token, down_token, out, pacc, *refs):
    f, t = lax.axis_index("fs"), lax.axis_index("tp")

    @pl.when(lax.rem(t, 2) == 1)
    def _():
        loop(n_fs - 1, lambda i: greet({"fs": lax.rem(f + 1 + i, n_fs)}))
        w = hidden.shape[1]
        tile = 512

        def add_last(s, seg):
            for j in range(s * seg, (s + 1) * seg, tile):
                down = held_down[held_down.shape[0] - w :, j : j + tile]
                product = jnp.dot(hidden[...], down, preferred_element_type=jnp.float32)
                pacc[:, j : j + tile] = parts[:, j : j + tile] + product

        reduce_rows(pacc, post, out, add_last, True, *refs)

    @pl.when(lax.rem(t, 2) == 0)
    def _():
        out[...] = early[...]


def store_kernel(src, dst, token, sems):
    count = sems.shape[0]
    size = src.shape[0] // count
    copies = [
        pltpu.make_async_copy(src.at[pl.ds(p * size, size)], dst.at[pl.ds(p * size, size)], sems.at[p])
        for p in range(count)
    ]
    for copy in copies:
        copy.start()
    token[...] = jnp.zeros_like(token)
    for copy in copies:
        copy.wait()


def store(array):
    return pl.pallas_call(
        store_kernel,
        out_shape=(jax.ShapeDtypeStruct(array.shape, array.dtype), jax.ShapeDtypeStruct((8, 128), jnp.float32)),
        in_specs=[pl.BlockSpec(memory_space=pltpu.VMEM)],
        out_specs=(pl.BlockSpec(memory_space=pl.ANY), pl.BlockSpec(memory_space=pltpu.VMEM)),
        scratch_shapes=[pltpu.SemaphoreType.DMA((STORES,))],
        compiler_params=pltpu.CompilerParams(vmem_limit_bytes=1000000),
    )(array)


def sum_kernel(n_fs, parts, gain, out, land, ss, rs):
    f = lax.axis_index("fs")

    def peer_of(i):
        return lax.rem(f + 1 + i, n_fs)

    loop(n_fs - 1, lambda i: greet({"fs": peer_of(i)}))
    pl.semaphore_wait(pltpu.get_barrier_semaphore(), n_fs - 1)

    def send(i):
        return remote(parts.at[peer_of(i)], land.at[f], ss.at[i], rs.at[f], {"fs": peer_of(i)})

    loop(n_fs - 1, lambda i: send(i).start())

    def add(i, total):
        source = peer_of(i)
        remote(land.at[source], land.at[source], ss.at[i], rs.at[source], {"fs": source}).wait_recv()
        return total + land[source].astype(jnp.float32)

    summed = lax.fori_loop(0, n_fs - 1, add, parts[f].astype(jnp.float32))
    scale = lax.rsqrt(jnp.mean(summed * summed, axis=-1, keepdims=True) + EPS)
    out[...] = (summed * scale * gain[...]).astype(out.dtype)
    loop(n_fs - 1, lambda i: send(i).wait_send())


def on_device(n_fs, n_tp, prompt_tokens, trained_up, trained_down, pre_gain, post_gain):
    bf16, f32 = jnp.bfloat16, jnp.float32
    rows, cols = trained_up.shape
    d_rows, d_cols = trained_down.shape
    tokens, width = prompt_tokens.shape[1:]
    m = n_fs // n_tp
    owned = cols // m
    w = min(owned, CHUNK)
    n_c = owned // w
    pieces = m * n_c
    share = tokens // n_fs
    q = GROUP
    n_o = n_fs // q
    seg = width // SEGMENTS
    fused = share % 16 == 0 and n_fs % q == 0 and n_o > 1
    anywhere = pl.BlockSpec(memory_space=pl.ANY)
    vmem = pl.BlockSpec(memory_space=pltpu.VMEM)
    dma = pltpu.SemaphoreType.DMA
    reduce_scratch = [
        pltpu.VMEM((SEGMENTS, q, n_o, share, seg), bf16),
        pltpu.VMEM((SEGMENTS, q, n_o, share, seg), bf16),
        pltpu.VMEM((SEGMENTS, n_o, share, seg), bf16),
        pltpu.VMEM((SEGMENTS, n_o, share, seg), bf16),
        pltpu.VMEM((share, width), f32),
        dma, dma((SEGMENTS, q)),
        dma, dma((SEGMENTS, n_o)),
    ]
    held_up, held_down, parts, hidden, early = pl.pallas_call(
        functools.partial(spread_kernel, n_fs, n_tp, w, fused),
        out_shape=(
            pltpu.VMEM((n_fs * rows, owned), bf16),
            pltpu.VMEM((d_rows, n_tp * d_cols), bf16),
            pltpu.VMEM((tokens, width), f32),
            pltpu.VMEM((tokens, w), bf16),
            jax.ShapeDtypeStruct((share, width), bf16),
        ),
        in_specs=[anywhere, anywhere, vmem, vmem, vmem],
        out_specs=(vmem, vmem, vmem, vmem, vmem),
        scratch_shapes=[
            pltpu.VMEM((min(DEPTH, pieces), rows, w), f32),
            pltpu.VMEM((2, d_rows // n_c, d_cols), f32),
            pltpu.VMEM((pieces, rows, w), bf16),
            pltpu.VMEM((pieces, rows, w), bf16),
            pltpu.VMEM((rows, 128), f32),
            pltpu.VMEM((n_fs, tokens, rows), bf16),
            pltpu.VMEM((tokens, w), f32),
            dma((min(DEPTH, pieces),)), dma((2,)),
            dma, dma((pieces + m * (PARTS - 1),)),
            dma((2,)), dma((n_fs, n_c)),
            dma, dma((n_fs, n_c)),
            dma, dma,
            dma, dma((n_c,)),
            dma, dma((n_c,)),
        ] + (reduce_scratch if fused else []),
        compiler_params=pltpu.CompilerParams(collective_id=0, has_side_effects=True, vmem_limit_bytes=30500000),
    )(trained_up, trained_down, prompt_tokens[0], pre_gain[None], post_gain[None])
    sampler_up, up_token = store(held_up)
    sampler_down, down_token = store(held_down)
    if fused:
        layer_out = pl.pallas_call(
            functools.partial(late_kernel, n_fs),
            out_shape=jax.ShapeDtypeStruct((share, width), bf16),
            in_specs=[vmem, vmem, vmem, vmem, vmem, anywhere, anywhere],
            out_specs=vmem,
            scratch_shapes=[pltpu.VMEM((tokens, width), f32)] + reduce_scratch,
            compiler_params=pltpu.CompilerParams(collective_id=1, has_side_effects=True, vmem_limit_bytes=16000000),
        )(parts, hidden, held_down, post_gain[None], early, up_token, down_token)
        return (layer_out[None], sampler_up, sampler_down)

    layer_out = pl.pallas_call(
        functools.partial(sum_kernel, n_fs),
        out_shape=jax.ShapeDtypeStruct((share, width), bf16),
        in_specs=[vmem, vmem],
        out_specs=vmem,
        scratch_shapes=[pltpu.VMEM((n_fs, share, width), bf16), dma((n_fs - 1,)), dma((n_fs,))],
        compiler_params=pltpu.CompilerParams(collective_id=1, has_side_effects=True, vmem_limit_bytes=16000000),
    )(parts.astype(bf16).reshape(n_fs, share, width), post_gain[None])
    return (layer_out[None], sampler_up, sampler_down)


def solution(mesh):
    placed = (P("tp", None, None), P("fs", "tp"), P("fs", "tp"), P("fs"), P())
    return jax.shard_map(
        functools.partial(on_device, mesh.shape["fs"], mesh.shape["tp"]),
        mesh=mesh,
        in_specs=placed,
        out_specs=(P("tp", "fs", None), P(None, "fs"), P("fs", None)),
        check_vma=False,
    )
```

```python
import functools

import jax
import jax.numpy as jnp
from jax import lax
from jax.experimental import pallas as pl
from jax.experimental.pallas import tpu as pltpu
from jax.sharding import PartitionSpec as P

MESH = pl.DeviceIdType.MESH
EPS = 1e-06
CHUNK = 256
SEGMENTS = 4
GROUP = 4
STORES = 4
PARTS = 4
DEPTH = 4


def remote(src, dst, send_sem, recv_sem, device):
    return pltpu.make_async_remote_copy(
        src_ref=src, dst_ref=dst, send_sem=send_sem, recv_sem=recv_sem, device_id=device, device_id_type=MESH
    )


def greet(device):
    pl.semaphore_signal(pltpu.get_barrier_semaphore(), inc=1, device_id=device, device_id_type=MESH)


def loop(count, body):
    lax.fori_loop(0, count, lambda i, c: (body(i), c)[1], 0)


def span(i, size):
    return pl.ds(pl.multiple_of(i * size, size), size)


def square_norm(values):
    return values * lax.rsqrt(jnp.mean(values * values, axis=-1, keepdims=True) + EPS)


def spread_kernel(
    n_fs, n_tp, w, fused,
    up_in, down_in, tokens, gain, post, held_up, held_down, pacc, hid, out,
    stage, dstage, upb, xup, gcol, normed, acc, us, ds_in,
    xs, xr, ps, pr, prf, ws, wr, wrf, ns, nr, ds, dr, vs, vr, *reduce_refs,
):
    f, t = lax.axis_index("fs"), lax.axis_index("tp")
    far = lax.rem(t + n_tp // 2, n_tp)
    near = t + 1 - 2 * lax.rem(t, 2)
    near_far = lax.rem(near + n_tp // 2, n_tp)
    m = n_fs // n_tp
    rows, cols = up_in.shape
    owned = cols // m
    d_rows, d_width = down_in.shape
    width = n_tp * d_width
    n_c = owned // w
    d_part = d_rows // n_c
    pieces = m * n_c
    block_of_f = f // m
    active = lax.rem(lax.rem(block_of_f, 2) + lax.rem(t, 2), 2) == 0

    depth = stage.shape[0]

    def load_up(k):
        return pltpu.make_async_copy(
            up_in.at[:, span(lax.rem(k, m) * n_c + k // m, w)], stage.at[lax.rem(k, depth)], us.at[lax.rem(k, depth)]
        )

    def load_down(c):
        return pltpu.make_async_copy(down_in.at[span(c, d_part)], dstage.at[lax.rem(c, 2)], ds_in.at[lax.rem(c, 2)])

    def landed(source, c):
        return held_up.at[span(source, rows), span(c, w)]

    half = n_fs // 2
    n_s = PARTS if rows % (16 * PARTS) == 0 else 1
    fine = n_s > 1 and n_c > 2
    closing = pieces - m if fine else pieces
    sub = rows // n_s

    def x_part(k, r):
        at = pl.ds(r * sub, sub)
        return remote(upb.at[k, at], xup.at[k, at], xs, xr.at[k * n_s + r], {"tp": far})

    def x_copy(k):
        return remote(upb.at[k], xup.at[k], xs, xr.at[m * (n_s - 1) + k], {"tp": far})

    def owner(phase, k):
        return (t if phase == 0 else far) * m + lax.rem(k, m)

    def landed_part(source, c, r):
        return held_up.at[pl.ds(pl.multiple_of(source * rows + r * sub, sub), sub), span(c, w)]

    def start_peer(phase, k, first, size, sem=None):
        to = owner(phase, k)
        held = (upb if phase == 0 else xup).at[k, pl.ds(first, size)]
        at = held_up.at[pl.ds(pl.multiple_of(f * rows + first, size), size), span(k // m, w)]
        if sem is None:
            sem = pr.at[lax.rem(f // half + to // half, 2), k // m]

        @pl.when(to != f)
        def _():
            remote(held, at, ps.at[phase], sem, {"fs": to}).start()

    def end_peers(phase):
        held = upb if phase == 0 else xup
        own = block_of_f == (t if phase == 0 else far)

        def ended(count):
            sent = held.at[pl.ds(0, count)]
            remote(sent, sent, ps.at[phase], ps.at[phase], {"tp": far}).wait_send()

        @pl.when(own)
        def _():
            ended(pieces - n_c)

        @pl.when(jnp.logical_not(own))
        def _():
            ended(pieces)

    def block(c, which):
        return held_down.at[span(c, d_part), span(which, d_width)]

    def d_copy(c):
        return remote(block(c, t), block(c, t), ds, dr.at[c], {"tp": far})

    def d_pass(c, which):
        return remote(block(c, which), block(c, which), vs, vr.at[c], {"tp": near})

    def column(which):
        return held_down.at[:, span(which, d_width)]

    def to_near(which):
        return remote(column(which), column(which), ns, nr, {"tp": near})

    loop(n_fs - 1, lambda i: greet({"fs": lax.rem(f + 1 + i, n_fs)}))
    greet({"tp": far})
    greet({"tp": near})
    loop(depth, lambda k: load_up(k).start())
    for c in range(min(2, n_c)):
        load_down(c).start()

    side = min(rows, 128)
    eye = lax.broadcasted_iota(jnp.int32, (side, side), 0) == lax.broadcasted_iota(jnp.int32, (side, side), 1)
    for b in range(rows // side):
        line = jnp.broadcast_to(gain[:, b * side : (b + 1) * side], (side, side))
        scale = jnp.sum(jnp.where(eye, line, 0.0), axis=1, keepdims=True)
        gcol[b * side : (b + 1) * side, :] = jnp.broadcast_to(scale, (side, 128))

    def convert(k):
        load_up(k).wait()
        for j in range(0, w, 128):
            upb[k, :, j : j + 128] = (gcol[...] * stage[lax.rem(k, depth), :, j : j + 128]).astype(upb.dtype)

        @pl.when(k + depth < pieces)
        def _():
            load_up(k + depth).start()

    def send_parts(k):
        for r in range(n_s):
            x_part(k, r).start()
        for r in range(n_s):
            start_peer(0, k, r * sub, sub)

    def send(k):
        x_copy(k).start()
        start_peer(0, k, 0, rows)

    convert(0)
    pl.semaphore_wait(pltpu.get_barrier_semaphore(), n_fs + 1)

    for k in range(min(m, pieces - 1)):
        convert(k + 1)
        send_parts(k)

    def send_closing(k):
        x_copy(k).start()
        for r in range(n_s):
            start_peer(0, k, r * sub, sub, prf.at[f, r])

    def convert_and_send(k):
        convert(k)
        send(k - 1)

    lax.fori_loop(m + 1, closing + 1 if fine else pieces, lambda k, c: (convert_and_send(k), c)[1], 0)
    for k in range(closing, pieces - 1):
        convert(k + 1)
        send_closing(k)
    pacc[...] = jnp.zeros_like(pacc)
    (send_closing if fine else send if pieces > m else send_parts)(pieces - 1)

    def convert_down(c):
        load_down(c).wait()
        held_down[span(c, d_part), span(t, d_width)] = dstage[lax.rem(c, 2)].astype(held_down.dtype)

        @pl.when(c + 2 < n_c)
        def _():
            load_down(c + 2).start()

    def between(k):
        @pl.when(k == max(pieces - 2, 0))
        def _():
            loop(n_c, lambda c: d_copy(c).start())
            to_near(t).start()

        @pl.when(k < n_c)
        def _():
            convert_down(k)

        @pl.when(k == n_c)
        def _():
            scaled = square_norm(tokens[...].astype(jnp.float32)).astype(jnp.bfloat16)
            for i in range(n_fs):
                normed[i] = scaled[:, i * rows : (i + 1) * rows]

    def pass_parts(k):
        for r in range(n_s):
            x_part(k, r).wait_recv()
            start_peer(1, k, r * sub, sub)
        between(k)

    def pass_on(k):
        x_copy(k).wait_recv()
        start_peer(1, k, 0, rows)
        between(k)

    def pass_closing(k):
        x_copy(k).wait_recv()
        for r in range(n_s):
            start_peer(1, k, r * sub, sub, prf.at[f, r])
        between(k)

    loop(m, pass_parts)
    lax.fori_loop(m, closing, lambda k, c: (pass_on(k), c)[1], 0)
    lax.fori_loop(closing, pieces, lambda k, c: (pass_closing(k), c)[1], 0)

    def gather(c, final):
        remote(block(c, far), block(c, far), ds, dr.at[c], {"tp": far}).wait_recv()
        d_pass(c, far).start()
        acc[...] = jnp.zeros_like(acc)
        mine = f // half

        def source_at(side, step):
            return lax.rem(mine + side, 2) * half + lax.rem(f + step, half)

        def rows_at(first, count):
            return held_up.at[pl.ds(pl.multiple_of(first * rows, rows), count * rows), span(c, w)]

        def side_rows(side):
            return rows_at(lax.rem(mine + side, 2) * half, half)

        def share(src, to, sem):
            return remote(src, to, ws, sem, {"tp": near})

        def share_sem(side, source):
            return wrf.at[source] if final else wr.at[side, c]

        def keep_own(held):
            k = c * m + lax.rem(f, m)
            share(held.at[k], rows_at(f, 1), share_sem(0, f)).start()
            held_up[span(f, rows), span(c, w)] = held[k]

        @pl.when(jnp.logical_and(active, block_of_f == t))
        def _():
            keep_own(upb)

        @pl.when(jnp.logical_and(active, block_of_f != t))
        def _():
            keep_own(xup)

        def pass_part(side, i):
            source, r = source_at(side, lax.rem(i, half)), i // half
            part = landed_part(source, c, r)
            share(part, part, prf.at[source, r]).wait_recv()
            share(part, part, wrf.at[source]).start()

        def add_up(source):
            acc[...] += jnp.dot(
                normed[source], held_up[span(source, rows), span(c, w)], preferred_element_type=jnp.float32
            )

        for side in range(2):
            @pl.when(active)
            def _():
                if final:
                    def one(i):
                        @pl.when(jnp.logical_or(side > 0, lax.rem(i, half) > 0))
                        def _():
                            pass_part(side, i)

                    loop(half * n_s, one)
                elif side == 0:
                    others = rows_at(0, half - 1)
                    share(others, others, pr.at[side, c]).wait_recv()

                    def one(i):
                        at = rows_at(source_at(side, i + 1), 1)
                        share(at, at, wr.at[side, c]).start()

                    loop(half - 1, one)
                else:
                    at = side_rows(side)
                    share(at, at, pr.at[side, c]).wait_recv()
                    share(at, at, wr.at[side, c]).start()

            if not final:
                @pl.when(jnp.logical_not(active))
                def _():
                    share(side_rows(side), side_rows(side), wr.at[side, c]).wait_recv()

            def close_one(step):
                source = source_at(side, step)
                if final:
                    @pl.when(jnp.logical_not(active))
                    def _():
                        share(rows_at(source, 1), rows_at(source, 1), wrf.at[source]).wait_recv()

                add_up(source)

            loop(half, close_one)

        hid[...] = jnp.square(jnp.maximum(acc[...], 0.0)).astype(jnp.bfloat16)
        d_pass(c, near_far).wait_recv()

        @pl.when(c == 0)
        def _():
            to_near(near).wait_recv()

    def add_down(c, first, count):
        tile = min(d_width, 512)

        def one(i):
            at = pl.ds(pl.multiple_of(first + i * tile, tile), tile)
            pacc[:, at] += jnp.dot(hid[...], held_down[span(c, d_part), at], preferred_element_type=jnp.float32)

        loop(count // tile, one)

    def whole_chunk(c):
        gather(c, False)
        add_down(c, 0, width)

    last = n_c - 1
    loop(last, whole_chunk)
    gather(last, fine)
    if fused:
        @pl.when(lax.rem(t, 2) == 0)
        def _():
            reduce_rows(pacc, post, out, lambda s, seg: add_down(last, s * seg, seg), False, *reduce_refs)
    else:
        add_down(last, 0, width)
        out[...] = jnp.zeros_like(out)

    @pl.when(active)
    def _():
        remote(held_up, held_up, ws, ws, {"tp": near}).wait_send()

    to_near(t).wait_send()
    remote(column(t), column(t), ds, ds, {"tp": far}).wait_send()
    remote(column(far), column(far), vs, vs, {"tp": near}).wait_send()
    remote(upb, xup, xs, xs, {"tp": far}).wait_send()
    end_peers(0)
    end_peers(1)


def reduce_rows(pacc, post, out, compute, waiting, sb, land, sb2, land2, fin, ss, rs, ss2, rs2):
    f = lax.axis_index("fs")
    _, q, n_o, part, seg = sb.shape
    i, o = lax.rem(f, q), f // q

    def peer(d):
        return lax.rem(i + d, q)

    def across(d):
        return lax.rem(o + d, n_o)

    def first_copy(s, d):
        return remote(sb.at[s, peer(d)], land.at[s, i], ss, rs.at[s], {"fs": o * q + peer(d)})

    def second_copy(s, d):
        return remote(sb2.at[s, across(d)], land2.at[s, o], ss2, rs2.at[s], {"fs": across(d) * q + i})

    ready = SEGMENTS // 2

    def fill(s):
        for b in range(n_o * q):
            sb[s, b % q, b // q] = pacc[b * part : (b + 1) * part, s * seg : (s + 1) * seg].astype(sb.dtype)

    def send(s):
        for d in range(1, q):
            first_copy(s, d).start()

    if waiting:
        for s in range(SEGMENTS):
            compute(s, seg)
            fill(s)
            if s == ready:
                pl.semaphore_wait(pltpu.get_barrier_semaphore(), n_o * q - 1)
                for r in range(s):
                    send(r)
            if s >= ready:
                send(s)
    else:
        for s in range(SEGMENTS):
            compute(s, seg)
            fill(s)
            send(s)

    for s in range(SEGMENTS):
        arrived = land.at[s, pl.ds(0, q - 1)]
        remote(arrived, arrived, ss, rs.at[s], {"fs": f}).wait_recv()

        def total(to):
            value = pacc[span(to * q + i, part), s * seg : (s + 1) * seg]
            for d in range(1, q):
                value += land[s, peer(d), to].astype(jnp.float32)
            return value

        for d in range(1, n_o):
            sb2[s, across(d)] = total(across(d)).astype(sb2.dtype)
        fin[:, s * seg : (s + 1) * seg] = total(o)
        for d in range(1, n_o):
            second_copy(s, d).start()

    for s in range(SEGMENTS):
        value = fin[:, s * seg : (s + 1) * seg]
        arrived = land2.at[s, pl.ds(0, n_o - 1)]
        remote(arrived, arrived, ss2, rs2.at[s], {"fs": f}).wait_recv()
        for d in range(1, n_o):
            value += land2[s, across(d)].astype(jnp.float32)
        fin[:, s * seg : (s + 1) * seg] = value
    summed = fin[...]
    scale = lax.rsqrt(jnp.mean(summed * summed, axis=-1, keepdims=True) + EPS)
    out[...] = (summed * scale * post[...]).astype(out.dtype)
    for buffer, count, sem in ((sb, q - 1, ss), (sb2, n_o - 1, ss2)):
        sent = buffer.at[:, pl.ds(0, count)]
        remote(sent, sent, sem, sem, {"fs": f}).wait_send()


def late_kernel(n_fs, parts, hidden, held_down, post, early, up_token, down_token, out, pacc, *refs):
    f, t = lax.axis_index("fs"), lax.axis_index("tp")

    @pl.when(lax.rem(t, 2) == 1)
    def _():
        loop(n_fs - 1, lambda i: greet({"fs": lax.rem(f + 1 + i, n_fs)}))
        w = hidden.shape[1]
        tile = 512

        def add_last(s, seg):
            for j in range(s * seg, (s + 1) * seg, tile):
                down = held_down[held_down.shape[0] - w :, j : j + tile]
                product = jnp.dot(hidden[...], down, preferred_element_type=jnp.float32)
                pacc[:, j : j + tile] = parts[:, j : j + tile] + product

        reduce_rows(pacc, post, out, add_last, True, *refs)

    @pl.when(lax.rem(t, 2) == 0)
    def _():
        out[...] = early[...]


def store_kernel(src, dst, token, sems):
    count = sems.shape[0]
    size = src.shape[0] // count
    copies = [
        pltpu.make_async_copy(src.at[pl.ds(p * size, size)], dst.at[pl.ds(p * size, size)], sems.at[p])
        for p in range(count)
    ]
    for copy in copies:
        copy.start()
    token[...] = jnp.zeros_like(token)
    for copy in copies:
        copy.wait()


def store(array):
    return pl.pallas_call(
        store_kernel,
        out_shape=(jax.ShapeDtypeStruct(array.shape, array.dtype), jax.ShapeDtypeStruct((8, 128), jnp.float32)),
        in_specs=[pl.BlockSpec(memory_space=pltpu.VMEM)],
        out_specs=(pl.BlockSpec(memory_space=pl.ANY), pl.BlockSpec(memory_space=pltpu.VMEM)),
        scratch_shapes=[pltpu.SemaphoreType.DMA((STORES,))],
        compiler_params=pltpu.CompilerParams(vmem_limit_bytes=1000000),
    )(array)


def sum_kernel(n_fs, parts, gain, out, land, ss, rs):
    f = lax.axis_index("fs")

    def peer_of(i):
        return lax.rem(f + 1 + i, n_fs)

    loop(n_fs - 1, lambda i: greet({"fs": peer_of(i)}))
    pl.semaphore_wait(pltpu.get_barrier_semaphore(), n_fs - 1)

    def send(i):
        return remote(parts.at[peer_of(i)], land.at[f], ss.at[i], rs.at[f], {"fs": peer_of(i)})

    loop(n_fs - 1, lambda i: send(i).start())

    def add(i, total):
        source = peer_of(i)
        remote(land.at[source], land.at[source], ss.at[i], rs.at[source], {"fs": source}).wait_recv()
        return total + land[source].astype(jnp.float32)

    summed = lax.fori_loop(0, n_fs - 1, add, parts[f].astype(jnp.float32))
    scale = lax.rsqrt(jnp.mean(summed * summed, axis=-1, keepdims=True) + EPS)
    out[...] = (summed * scale * gain[...]).astype(out.dtype)
    loop(n_fs - 1, lambda i: send(i).wait_send())


def on_device(n_fs, n_tp, prompt_tokens, trained_up, trained_down, pre_gain, post_gain):
    bf16, f32 = jnp.bfloat16, jnp.float32
    rows, cols = trained_up.shape
    d_rows, d_cols = trained_down.shape
    tokens, width = prompt_tokens.shape[1:]
    m = n_fs // n_tp
    owned = cols // m
    w = min(owned, CHUNK)
    n_c = owned // w
    pieces = m * n_c
    share = tokens // n_fs
    q = GROUP
    n_o = n_fs // q
    seg = width // SEGMENTS
    fused = share % 16 == 0 and n_fs % q == 0 and n_o > 1
    anywhere = pl.BlockSpec(memory_space=pl.ANY)
    vmem = pl.BlockSpec(memory_space=pltpu.VMEM)
    dma = pltpu.SemaphoreType.DMA
    reduce_scratch = [
        pltpu.VMEM((SEGMENTS, q, n_o, share, seg), bf16),
        pltpu.VMEM((SEGMENTS, q, n_o, share, seg), bf16),
        pltpu.VMEM((SEGMENTS, n_o, share, seg), bf16),
        pltpu.VMEM((SEGMENTS, n_o, share, seg), bf16),
        pltpu.VMEM((share, width), f32),
        dma, dma((SEGMENTS,)),
        dma, dma((SEGMENTS,)),
    ]
    held_up, held_down, parts, hidden, early = pl.pallas_call(
        functools.partial(spread_kernel, n_fs, n_tp, w, fused),
        out_shape=(
            pltpu.VMEM((n_fs * rows, owned), bf16),
            pltpu.VMEM((d_rows, n_tp * d_cols), bf16),
            pltpu.VMEM((tokens, width), f32),
            pltpu.VMEM((tokens, w), bf16),
            jax.ShapeDtypeStruct((share, width), bf16),
        ),
        in_specs=[anywhere, anywhere, vmem, vmem, vmem],
        out_specs=(vmem, vmem, vmem, vmem, vmem),
        scratch_shapes=[
            pltpu.VMEM((min(DEPTH, pieces), rows, w), f32),
            pltpu.VMEM((2, d_rows // n_c, d_cols), f32),
            pltpu.VMEM((pieces, rows, w), bf16),
            pltpu.VMEM((pieces, rows, w), bf16),
            pltpu.VMEM((rows, 128), f32),
            pltpu.VMEM((n_fs, tokens, rows), bf16),
            pltpu.VMEM((tokens, w), f32),
            dma((min(DEPTH, pieces),)), dma((2,)),
            dma, dma((pieces + m * (PARTS - 1),)),
            dma((2,)), dma((2, n_c)), dma((n_fs, PARTS)),
            dma, dma((2, n_c)), dma((n_fs,)),
            dma, dma,
            dma, dma((n_c,)),
            dma, dma((n_c,)),
        ] + (reduce_scratch if fused else []),
        compiler_params=pltpu.CompilerParams(collective_id=0, has_side_effects=True, vmem_limit_bytes=30500000),
    )(trained_up, trained_down, prompt_tokens[0], pre_gain[None], post_gain[None])
    sampler_up, up_token = store(held_up)
    sampler_down, down_token = store(held_down)
    if fused:
        layer_out = pl.pallas_call(
            functools.partial(late_kernel, n_fs),
            out_shape=jax.ShapeDtypeStruct((share, width), bf16),
            in_specs=[vmem, vmem, vmem, vmem, vmem, anywhere, anywhere],
            out_specs=vmem,
            scratch_shapes=[pltpu.VMEM((tokens, width), f32)] + reduce_scratch,
            compiler_params=pltpu.CompilerParams(collective_id=1, has_side_effects=True, vmem_limit_bytes=16000000),
        )(parts, hidden, held_down, post_gain[None], early, up_token, down_token)
        return (layer_out[None], sampler_up, sampler_down)

    layer_out = pl.pallas_call(
        functools.partial(sum_kernel, n_fs),
        out_shape=jax.ShapeDtypeStruct((share, width), bf16),
        in_specs=[vmem, vmem],
        out_specs=vmem,
        scratch_shapes=[pltpu.VMEM((n_fs, share, width), bf16), dma((n_fs - 1,)), dma((n_fs,))],
        compiler_params=pltpu.CompilerParams(collective_id=1, has_side_effects=True, vmem_limit_bytes=16000000),
    )(parts.astype(bf16).reshape(n_fs, share, width), post_gain[None])
    return (layer_out[None], sampler_up, sampler_down)


def solution(mesh):
    placed = (P("tp", None, None), P("fs", "tp"), P("fs", "tp"), P("fs"), P())
    return jax.shard_map(
        functools.partial(on_device, mesh.shape["fs"], mesh.shape["tp"]),
        mesh=mesh,
        in_specs=placed,
        out_specs=(P("tp", "fs", None), P(None, "fs"), P("fs", None)),
        check_vma=False,
    )
```

```python
import functools

import jax
import jax.numpy as jnp
from jax import lax
from jax.experimental import pallas as pl
from jax.experimental.pallas import tpu as pltpu
from jax.sharding import PartitionSpec as P

MESH = pl.DeviceIdType.MESH
EPS = 1e-06
CHUNK = 256
SEGMENTS = 4
GROUP = 4
STORES = 4
PARTS = 4
DEPTH = 4


def remote(src, dst, send_sem, recv_sem, device):
    return pltpu.make_async_remote_copy(
        src_ref=src, dst_ref=dst, send_sem=send_sem, recv_sem=recv_sem, device_id=device, device_id_type=MESH
    )


def greet(device):
    pl.semaphore_signal(pltpu.get_barrier_semaphore(), inc=1, device_id=device, device_id_type=MESH)


def loop(count, body):
    lax.fori_loop(0, count, lambda i, c: (body(i), c)[1], 0)


def span(i, size):
    return pl.ds(pl.multiple_of(i * size, size), size)


def square_norm(values):
    return values * lax.rsqrt(jnp.mean(values * values, axis=-1, keepdims=True) + EPS)


def spread_kernel(
    n_fs, n_tp, w, fused,
    up_in, down_in, tokens, gain, post, held_up, held_down, pacc, hid, out,
    stage, dstage, upb, xup, gcol, normed, acc, us, ds_in,
    xs, xr, ps, pr, prf, ws, wr, wrf, ns, nr, ds, dr, vs, vr, *reduce_refs,
):
    f, t = lax.axis_index("fs"), lax.axis_index("tp")
    far = lax.rem(t + n_tp // 2, n_tp)
    near = t + 1 - 2 * lax.rem(t, 2)
    near_far = lax.rem(near + n_tp // 2, n_tp)
    m = n_fs // n_tp
    rows, cols = up_in.shape
    owned = cols // m
    d_rows, d_width = down_in.shape
    width = n_tp * d_width
    n_c = owned // w
    d_part = d_rows // n_c
    pieces = m * n_c
    block_of_f = f // m
    active = lax.rem(lax.rem(block_of_f, 2) + lax.rem(t, 2), 2) == 0

    depth = stage.shape[0]

    def load_up(k):
        return pltpu.make_async_copy(
            up_in.at[:, span(lax.rem(k, m) * n_c + k // m, w)], stage.at[lax.rem(k, depth)], us.at[lax.rem(k, depth)]
        )

    def load_down(c):
        return pltpu.make_async_copy(down_in.at[span(c, d_part)], dstage.at[lax.rem(c, 2)], ds_in.at[lax.rem(c, 2)])

    def landed(source, c):
        return held_up.at[span(source, rows), span(c, w)]

    half = n_fs // 2
    n_s = PARTS if rows % (16 * PARTS) == 0 else 1
    fine = n_s > 1 and n_c > 2
    closing = pieces - m if fine else pieces
    sub = rows // n_s

    def x_part(k, r):
        at = pl.ds(r * sub, sub)
        return remote(upb.at[k, at], xup.at[k, at], xs, xr.at[k * n_s + r], {"tp": far})

    def x_copy(k):
        return remote(upb.at[k], xup.at[k], xs, xr.at[m * (n_s - 1) + k], {"tp": far})

    def owner(phase, k):
        return (t if phase == 0 else far) * m + lax.rem(k, m)

    def landed_part(source, c, r):
        return held_up.at[pl.ds(pl.multiple_of(source * rows + r * sub, sub), sub), span(c, w)]

    def start_peer(phase, k, first, size, sem=None):
        to = owner(phase, k)
        held = (upb if phase == 0 else xup).at[k, pl.ds(first, size)]
        at = held_up.at[pl.ds(pl.multiple_of(f * rows + first, size), size), span(k // m, w)]
        if sem is None:
            sem = pr.at[lax.rem(f // half + to // half, 2), k // m]

        @pl.when(to != f)
        def _():
            remote(held, at, ps.at[phase], sem, {"fs": to}).start()

    def end_peers(phase):
        held = upb if phase == 0 else xup
        own = block_of_f == (t if phase == 0 else far)

        def ended(count):
            sent = held.at[pl.ds(0, count)]
            remote(sent, sent, ps.at[phase], ps.at[phase], {"tp": far}).wait_send()

        @pl.when(own)
        def _():
            ended(pieces - n_c)

        @pl.when(jnp.logical_not(own))
        def _():
            ended(pieces)

    def block(c, which):
        return held_down.at[span(c, d_part), span(which, d_width)]

    def d_copy(c):
        return remote(block(c, t), block(c, t), ds, dr.at[c], {"tp": far})

    def d_pass(c, which):
        return remote(block(c, which), block(c, which), vs, vr.at[c], {"tp": near})

    def column(which):
        return held_down.at[:, span(which, d_width)]

    def to_near(which):
        return remote(column(which), column(which), ns, nr, {"tp": near})

    loop(n_fs - 1, lambda i: greet({"fs": lax.rem(f + 1 + i, n_fs)}))
    greet({"tp": far})
    greet({"tp": near})
    loop(depth, lambda k: load_up(k).start())
    for c in range(min(2, n_c)):
        load_down(c).start()

    side = min(rows, 128)
    eye = lax.broadcasted_iota(jnp.int32, (side, side), 0) == lax.broadcasted_iota(jnp.int32, (side, side), 1)
    for b in range(rows // side):
        line = jnp.broadcast_to(gain[:, b * side : (b + 1) * side], (side, side))
        scale = jnp.sum(jnp.where(eye, line, 0.0), axis=1, keepdims=True)
        gcol[b * side : (b + 1) * side, :] = jnp.broadcast_to(scale, (side, 128))

    def convert(k):
        load_up(k).wait()
        for j in range(0, w, 128):
            upb[k, :, j : j + 128] = (gcol[...] * stage[lax.rem(k, depth), :, j : j + 128]).astype(upb.dtype)

        @pl.when(k + depth < pieces)
        def _():
            load_up(k + depth).start()

    def send_parts(k):
        for r in range(n_s):
            x_part(k, r).start()
        for r in range(n_s):
            start_peer(0, k, r * sub, sub)

    def send(k):
        x_copy(k).start()
        start_peer(0, k, 0, rows)

    convert(0)
    pl.semaphore_wait(pltpu.get_barrier_semaphore(), n_fs + 1)

    for k in range(min(m, pieces - 1)):
        convert(k + 1)
        send_parts(k)

    def send_closing(k):
        x_copy(k).start()
        for r in range(n_s):
            start_peer(0, k, r * sub, sub, prf.at[f, r])

    def convert_and_send(k):
        convert(k)
        send(k - 1)

    lax.fori_loop(m + 1, closing + 1 if fine else pieces, lambda k, c: (convert_and_send(k), c)[1], 0)
    for k in range(closing, pieces - 1):
        convert(k + 1)
        send_closing(k)
    pacc[...] = jnp.zeros_like(pacc)
    (send_closing if fine else send if pieces > m else send_parts)(pieces - 1)

    def convert_down(c):
        load_down(c).wait()
        held_down[span(c, d_part), span(t, d_width)] = dstage[lax.rem(c, 2)].astype(held_down.dtype)

        @pl.when(c + 2 < n_c)
        def _():
            load_down(c + 2).start()

    def between(k):
        @pl.when(k == max(pieces - 2, 0))
        def _():
            loop(n_c, lambda c: d_copy(c).start())
            to_near(t).start()

        @pl.when(k < n_c)
        def _():
            convert_down(k)

        @pl.when(k == n_c)
        def _():
            scaled = square_norm(tokens[...].astype(jnp.float32)).astype(jnp.bfloat16)
            for i in range(n_fs):
                normed[i] = scaled[:, i * rows : (i + 1) * rows]

    def pass_parts(k):
        for r in range(n_s):
            x_part(k, r).wait_recv()
            start_peer(1, k, r * sub, sub)
        between(k)

    def pass_on(k):
        x_copy(k).wait_recv()
        start_peer(1, k, 0, rows)
        between(k)

    def pass_closing(k):
        x_copy(k).wait_recv()
        for r in range(n_s):
            start_peer(1, k, r * sub, sub, prf.at[f, r])
        between(k)

    loop(m, pass_parts)
    lax.fori_loop(m, closing, lambda k, c: (pass_on(k), c)[1], 0)
    lax.fori_loop(closing, pieces, lambda k, c: (pass_closing(k), c)[1], 0)

    def gather(c, final):
        def pass_down():
            remote(block(c, far), block(c, far), ds, dr.at[c], {"tp": far}).wait_recv()
            d_pass(c, far).start()

        if not final:
            pass_down()
        acc[...] = jnp.zeros_like(acc)
        mine = f // half

        def source_at(side, step):
            return lax.rem(mine + side, 2) * half + lax.rem(f + step, half)

        def rows_at(first, count):
            return held_up.at[pl.ds(pl.multiple_of(first * rows, rows), count * rows), span(c, w)]

        def side_rows(side):
            return rows_at(lax.rem(mine + side, 2) * half, half)

        def share(src, to, sem):
            return remote(src, to, ws, sem, {"tp": near})

        def share_sem(side, source):
            return wrf.at[source] if final else wr.at[side, c]

        def keep_own(held):
            k = c * m + lax.rem(f, m)
            share(held.at[k], rows_at(f, 1), share_sem(0, f)).start()
            held_up[span(f, rows), span(c, w)] = held[k]

        @pl.when(jnp.logical_and(active, block_of_f == t))
        def _():
            keep_own(upb)

        @pl.when(jnp.logical_and(active, block_of_f != t))
        def _():
            keep_own(xup)

        def pass_part(side, i):
            source, r = source_at(side, lax.rem(i, half)), i // half
            part = landed_part(source, c, r)
            share(part, part, prf.at[source, r]).wait_recv()
            share(part, part, wrf.at[source]).start()

        def add_up(source):
            acc[...] += jnp.dot(
                normed[source], held_up[span(source, rows), span(c, w)], preferred_element_type=jnp.float32
            )

        for side in range(2):
            if final and side == 1:
                pass_down()

            @pl.when(active)
            def _():
                if final:
                    def one(i):
                        @pl.when(jnp.logical_or(side > 0, lax.rem(i, half) > 0))
                        def _():
                            pass_part(side, i)

                    loop(half * n_s, one)
                elif side == 0:
                    others = rows_at(0, half - 1)
                    share(others, others, pr.at[side, c]).wait_recv()

                    def one(i):
                        at = rows_at(source_at(side, i + 1), 1)
                        share(at, at, wr.at[side, c]).start()

                    loop(half - 1, one)
                else:
                    at = side_rows(side)
                    share(at, at, pr.at[side, c]).wait_recv()
                    share(at, at, wr.at[side, c]).start()

            if not final:
                @pl.when(jnp.logical_not(active))
                def _():
                    share(side_rows(side), side_rows(side), wr.at[side, c]).wait_recv()

            def close_one(step):
                source = source_at(side, step)
                if final:
                    @pl.when(jnp.logical_not(active))
                    def _():
                        share(rows_at(source, 1), rows_at(source, 1), wrf.at[source]).wait_recv()

                add_up(source)

            loop(half, close_one)

        hid[...] = jnp.square(jnp.maximum(acc[...], 0.0)).astype(jnp.bfloat16)
        d_pass(c, near_far).wait_recv()

        @pl.when(c == 0)
        def _():
            to_near(near).wait_recv()

    def add_down(c, first, count):
        tile = min(d_width, 512)

        def one(i):
            at = pl.ds(pl.multiple_of(first + i * tile, tile), tile)
            pacc[:, at] += jnp.dot(hid[...], held_down[span(c, d_part), at], preferred_element_type=jnp.float32)

        loop(count // tile, one)

    def whole_chunk(c):
        gather(c, False)
        add_down(c, 0, width)

    last = n_c - 1
    loop(last, whole_chunk)
    gather(last, fine)
    if fused:
        @pl.when(lax.rem(t, 2) == 0)
        def _():
            reduce_rows(pacc, post, out, lambda s, seg: add_down(last, s * seg, seg), False, *reduce_refs)
    else:
        add_down(last, 0, width)
        out[...] = jnp.zeros_like(out)

    @pl.when(active)
    def _():
        remote(held_up, held_up, ws, ws, {"tp": near}).wait_send()

    to_near(t).wait_send()
    remote(column(t), column(t), ds, ds, {"tp": far}).wait_send()
    remote(column(far), column(far), vs, vs, {"tp": near}).wait_send()
    remote(upb, xup, xs, xs, {"tp": far}).wait_send()
    end_peers(0)
    end_peers(1)


def reduce_rows(pacc, post, out, compute, waiting, sb, land, sb2, land2, fin, ss, rs, ss2, rs2):
    f = lax.axis_index("fs")
    _, q, n_o, part, seg = sb.shape
    i, o = lax.rem(f, q), f // q

    def peer(d):
        return lax.rem(i + d, q)

    def across(d):
        return lax.rem(o + d, n_o)

    def first_copy(s, d):
        return remote(sb.at[s, peer(d)], land.at[s, i], ss, rs.at[s], {"fs": o * q + peer(d)})

    def second_copy(s, d):
        return remote(sb2.at[s, across(d)], land2.at[s, o], ss2, rs2.at[s], {"fs": across(d) * q + i})

    ready = SEGMENTS // 4

    def fill(s):
        for b in range(n_o * q):
            sb[s, b % q, b // q] = pacc[b * part : (b + 1) * part, s * seg : (s + 1) * seg].astype(sb.dtype)

    def send(s):
        for d in range(1, q):
            first_copy(s, d).start()

    if waiting:
        for s in range(SEGMENTS):
            compute(s, seg)
            fill(s)
            if s == ready:
                pl.semaphore_wait(pltpu.get_barrier_semaphore(), q - 1 + n_o - 1)
                for r in range(s):
                    send(r)
            if s >= ready:
                send(s)
    else:
        for s in range(SEGMENTS):
            compute(s, seg)
            fill(s)
            send(s)

    for s in range(SEGMENTS):
        arrived = land.at[s, pl.ds(0, q - 1)]
        remote(arrived, arrived, ss, rs.at[s], {"fs": f}).wait_recv()

        def total(to):
            value = pacc[span(to * q + i, part), s * seg : (s + 1) * seg]
            for d in range(1, q):
                value += land[s, peer(d), to].astype(jnp.float32)
            return value

        for d in range(1, n_o):
            sb2[s, across(d)] = total(across(d)).astype(sb2.dtype)
        fin[:, s * seg : (s + 1) * seg] = total(o)
        for d in range(1, n_o):
            second_copy(s, d).start()

    for s in range(SEGMENTS):
        value = fin[:, s * seg : (s + 1) * seg]
        arrived = land2.at[s, pl.ds(0, n_o - 1)]
        remote(arrived, arrived, ss2, rs2.at[s], {"fs": f}).wait_recv()
        for d in range(1, n_o):
            value += land2[s, across(d)].astype(jnp.float32)
        fin[:, s * seg : (s + 1) * seg] = value
    summed = fin[...]
    scale = lax.rsqrt(jnp.mean(summed * summed, axis=-1, keepdims=True) + EPS)
    out[...] = (summed * scale * post[...]).astype(out.dtype)
    for buffer, count, sem in ((sb, q - 1, ss), (sb2, n_o - 1, ss2)):
        sent = buffer.at[:, pl.ds(0, count)]
        remote(sent, sent, sem, sem, {"fs": f}).wait_send()


def late_kernel(n_fs, parts, hidden, held_down, post, early, up_token, down_token, out, pacc, *refs):
    f, t = lax.axis_index("fs"), lax.axis_index("tp")

    @pl.when(lax.rem(t, 2) == 1)
    def _():
        _, q, n_o, _, _ = refs[0].shape
        i, o = lax.rem(f, q), f // q
        for d in range(1, q):
            greet({"fs": o * q + lax.rem(i + d, q)})
        for d in range(1, n_o):
            greet({"fs": lax.rem(o + d, n_o) * q + i})
        w = hidden.shape[1]
        tile = 512

        def add_last(s, seg):
            for j in range(s * seg, (s + 1) * seg, tile):
                down = held_down[held_down.shape[0] - w :, j : j + tile]
                product = jnp.dot(hidden[...], down, preferred_element_type=jnp.float32)
                pacc[:, j : j + tile] = parts[:, j : j + tile] + product

        reduce_rows(pacc, post, out, add_last, True, *refs)

    @pl.when(lax.rem(t, 2) == 0)
    def _():
        out[...] = early[...]


def store_kernel(src, dst, token, sems):
    count = sems.shape[0]
    size = src.shape[0] // count
    copies = [
        pltpu.make_async_copy(src.at[pl.ds(p * size, size)], dst.at[pl.ds(p * size, size)], sems.at[p])
        for p in range(count)
    ]
    for copy in copies:
        copy.start()
    token[...] = jnp.zeros_like(token)
    for copy in copies:
        copy.wait()


def store(array):
    return pl.pallas_call(
        store_kernel,
        out_shape=(jax.ShapeDtypeStruct(array.shape, array.dtype), jax.ShapeDtypeStruct((8, 128), jnp.float32)),
        in_specs=[pl.BlockSpec(memory_space=pltpu.VMEM)],
        out_specs=(pl.BlockSpec(memory_space=pl.ANY), pl.BlockSpec(memory_space=pltpu.VMEM)),
        scratch_shapes=[pltpu.SemaphoreType.DMA((STORES,))],
        compiler_params=pltpu.CompilerParams(vmem_limit_bytes=1000000),
    )(array)


def sum_kernel(n_fs, parts, gain, out, land, ss, rs):
    f = lax.axis_index("fs")

    def peer_of(i):
        return lax.rem(f + 1 + i, n_fs)

    loop(n_fs - 1, lambda i: greet({"fs": peer_of(i)}))
    pl.semaphore_wait(pltpu.get_barrier_semaphore(), n_fs - 1)

    def send(i):
        return remote(parts.at[peer_of(i)], land.at[f], ss.at[i], rs.at[f], {"fs": peer_of(i)})

    loop(n_fs - 1, lambda i: send(i).start())

    def add(i, total):
        source = peer_of(i)
        remote(land.at[source], land.at[source], ss.at[i], rs.at[source], {"fs": source}).wait_recv()
        return total + land[source].astype(jnp.float32)

    summed = lax.fori_loop(0, n_fs - 1, add, parts[f].astype(jnp.float32))
    scale = lax.rsqrt(jnp.mean(summed * summed, axis=-1, keepdims=True) + EPS)
    out[...] = (summed * scale * gain[...]).astype(out.dtype)
    loop(n_fs - 1, lambda i: send(i).wait_send())


def on_device(n_fs, n_tp, prompt_tokens, trained_up, trained_down, pre_gain, post_gain):
    bf16, f32 = jnp.bfloat16, jnp.float32
    rows, cols = trained_up.shape
    d_rows, d_cols = trained_down.shape
    tokens, width = prompt_tokens.shape[1:]
    m = n_fs // n_tp
    owned = cols // m
    w = min(owned, CHUNK)
    n_c = owned // w
    pieces = m * n_c
    share = tokens // n_fs
    q = GROUP
    n_o = n_fs // q
    seg = width // SEGMENTS
    fused = share % 16 == 0 and n_fs % q == 0 and n_o > 1
    anywhere = pl.BlockSpec(memory_space=pl.ANY)
    vmem = pl.BlockSpec(memory_space=pltpu.VMEM)
    dma = pltpu.SemaphoreType.DMA
    reduce_scratch = [
        pltpu.VMEM((SEGMENTS, q, n_o, share, seg), bf16),
        pltpu.VMEM((SEGMENTS, q, n_o, share, seg), bf16),
        pltpu.VMEM((SEGMENTS, n_o, share, seg), bf16),
        pltpu.VMEM((SEGMENTS, n_o, share, seg), bf16),
        pltpu.VMEM((share, width), f32),
        dma, dma((SEGMENTS,)),
        dma, dma((SEGMENTS,)),
    ]
    held_up, held_down, parts, hidden, early = pl.pallas_call(
        functools.partial(spread_kernel, n_fs, n_tp, w, fused),
        out_shape=(
            pltpu.VMEM((n_fs * rows, owned), bf16),
            pltpu.VMEM((d_rows, n_tp * d_cols), bf16),
            pltpu.VMEM((tokens, width), f32),
            pltpu.VMEM((tokens, w), bf16),
            jax.ShapeDtypeStruct((share, width), bf16),
        ),
        in_specs=[anywhere, anywhere, vmem, vmem, vmem],
        out_specs=(vmem, vmem, vmem, vmem, vmem),
        scratch_shapes=[
            pltpu.VMEM((min(DEPTH, pieces), rows, w), f32),
            pltpu.VMEM((2, d_rows // n_c, d_cols), f32),
            pltpu.VMEM((pieces, rows, w), bf16),
            pltpu.VMEM((pieces, rows, w), bf16),
            pltpu.VMEM((rows, 128), f32),
            pltpu.VMEM((n_fs, tokens, rows), bf16),
            pltpu.VMEM((tokens, w), f32),
            dma((min(DEPTH, pieces),)), dma((2,)),
            dma, dma((pieces + m * (PARTS - 1),)),
            dma((2,)), dma((2, n_c)), dma((n_fs, PARTS)),
            dma, dma((2, n_c)), dma((n_fs,)),
            dma, dma,
            dma, dma((n_c,)),
            dma, dma((n_c,)),
        ] + (reduce_scratch if fused else []),
        compiler_params=pltpu.CompilerParams(collective_id=0, has_side_effects=True, vmem_limit_bytes=30500000),
    )(trained_up, trained_down, prompt_tokens[0], pre_gain[None], post_gain[None])
    sampler_up, up_token = store(held_up)
    sampler_down, down_token = store(held_down)
    if fused:
        layer_out = pl.pallas_call(
            functools.partial(late_kernel, n_fs),
            out_shape=jax.ShapeDtypeStruct((share, width), bf16),
            in_specs=[vmem, vmem, vmem, vmem, vmem, anywhere, anywhere],
            out_specs=vmem,
            scratch_shapes=[pltpu.VMEM((tokens, width), f32)] + reduce_scratch,
            compiler_params=pltpu.CompilerParams(collective_id=1, has_side_effects=True, vmem_limit_bytes=16000000),
        )(parts, hidden, held_down, post_gain[None], early, up_token, down_token)
        return (layer_out[None], sampler_up, sampler_down)

    layer_out = pl.pallas_call(
        functools.partial(sum_kernel, n_fs),
        out_shape=jax.ShapeDtypeStruct((share, width), bf16),
        in_specs=[vmem, vmem],
        out_specs=vmem,
        scratch_shapes=[pltpu.VMEM((n_fs, share, width), bf16), dma((n_fs - 1,)), dma((n_fs,))],
        compiler_params=pltpu.CompilerParams(collective_id=1, has_side_effects=True, vmem_limit_bytes=16000000),
    )(parts.astype(bf16).reshape(n_fs, share, width), post_gain[None])
    return (layer_out[None], sampler_up, sampler_down)


def solution(mesh):
    placed = (P("tp", None, None), P("fs", "tp"), P("fs", "tp"), P("fs"), P())
    return jax.shard_map(
        functools.partial(on_device, mesh.shape["fs"], mesh.shape["tp"]),
        mesh=mesh,
        in_specs=placed,
        out_specs=(P("tp", "fs", None), P(None, "fs"), P("fs", None)),
        check_vma=False,
    )
```

```python
import functools

import jax
import jax.numpy as jnp
from jax import lax
from jax.experimental import pallas as pl
from jax.experimental.pallas import tpu as pltpu
from jax.sharding import PartitionSpec as P

MESH = pl.DeviceIdType.MESH
EPS = 1e-06
CHUNK = 256
SEGMENTS = 8
GROUP = 2
STORES = 4
PARTS = 4
DEPTH = 4


def remote(src, dst, send_sem, recv_sem, device):
    return pltpu.make_async_remote_copy(
        src_ref=src, dst_ref=dst, send_sem=send_sem, recv_sem=recv_sem, device_id=device, device_id_type=MESH
    )


def greet(device):
    pl.semaphore_signal(pltpu.get_barrier_semaphore(), inc=1, device_id=device, device_id_type=MESH)


def loop(count, body):
    lax.fori_loop(0, count, lambda i, c: (body(i), c)[1], 0)


def span(i, size):
    return pl.ds(pl.multiple_of(i * size, size), size)


def square_norm(values):
    return values * lax.rsqrt(jnp.mean(values * values, axis=-1, keepdims=True) + EPS)


def spread_kernel(
    n_fs, n_tp, w, fused,
    up_in, down_in, tokens, gain, post, held_up, held_down, pacc, hid, out,
    stage, dstage, upb, xup, gcol, normed, acc, us, ds_in,
    xs, xr, ps, pr, prf, ws, wr, wrf, ns, nr, ds, dr, vs, vr, *reduce_refs,
):
    f, t = lax.axis_index("fs"), lax.axis_index("tp")
    far = lax.rem(t + n_tp // 2, n_tp)
    near = t + 1 - 2 * lax.rem(t, 2)
    near_far = lax.rem(near + n_tp // 2, n_tp)
    m = n_fs // n_tp
    rows, cols = up_in.shape
    owned = cols // m
    d_rows, d_width = down_in.shape
    width = n_tp * d_width
    n_c = owned // w
    d_part = d_rows // n_c
    pieces = m * n_c
    block_of_f = f // m
    active = lax.rem(lax.rem(block_of_f, 2) + lax.rem(t, 2), 2) == 0

    depth = stage.shape[0]

    def load_up(k):
        return pltpu.make_async_copy(
            up_in.at[:, span(lax.rem(k, m) * n_c + k // m, w)], stage.at[lax.rem(k, depth)], us.at[lax.rem(k, depth)]
        )

    def load_down(c):
        return pltpu.make_async_copy(down_in.at[span(c, d_part)], dstage.at[lax.rem(c, 2)], ds_in.at[lax.rem(c, 2)])

    def landed(source, c):
        return held_up.at[span(source, rows), span(c, w)]

    half = n_fs // 2
    n_s = PARTS if rows % (16 * PARTS) == 0 else 1
    fine = n_s > 1 and n_c > 2
    closing = pieces - m if fine else pieces
    sub = rows // n_s

    def x_part(k, r):
        at = pl.ds(r * sub, sub)
        return remote(upb.at[k, at], xup.at[k, at], xs, xr.at[k * n_s + r], {"tp": far})

    def x_copy(k):
        return remote(upb.at[k], xup.at[k], xs, xr.at[m * (n_s - 1) + k], {"tp": far})

    def owner(phase, k):
        return (t if phase == 0 else far) * m + lax.rem(k, m)

    def landed_part(source, c, r):
        return held_up.at[pl.ds(pl.multiple_of(source * rows + r * sub, sub), sub), span(c, w)]

    def start_peer(phase, k, first, size, sem=None):
        to = owner(phase, k)
        held = (upb if phase == 0 else xup).at[k, pl.ds(first, size)]
        at = held_up.at[pl.ds(pl.multiple_of(f * rows + first, size), size), span(k // m, w)]
        if sem is None:
            sem = pr.at[lax.rem(f // half + to // half, 2), k // m]

        @pl.when(to != f)
        def _():
            remote(held, at, ps.at[phase], sem, {"fs": to}).start()

    def end_peers(phase):
        held = upb if phase == 0 else xup
        own = block_of_f == (t if phase == 0 else far)

        def ended(count):
            sent = held.at[pl.ds(0, count)]
            remote(sent, sent, ps.at[phase], ps.at[phase], {"tp": far}).wait_send()

        @pl.when(own)
        def _():
            ended(pieces - n_c)

        @pl.when(jnp.logical_not(own))
        def _():
            ended(pieces)

    def block(c, which):
        return held_down.at[span(c, d_part), span(which, d_width)]

    def d_copy(c):
        return remote(block(c, t), block(c, t), ds, dr.at[c], {"tp": far})

    def d_pass(c, which):
        return remote(block(c, which), block(c, which), vs, vr.at[c], {"tp": near})

    def column(which):
        return held_down.at[:, span(which, d_width)]

    def to_near(which):
        return remote(column(which), column(which), ns, nr, {"tp": near})

    loop(n_fs - 1, lambda i: greet({"fs": lax.rem(f + 1 + i, n_fs)}))
    greet({"tp": far})
    greet({"tp": near})
    loop(depth, lambda k: load_up(k).start())
    for c in range(min(2, n_c)):
        load_down(c).start()

    side = min(rows, 128)
    eye = lax.broadcasted_iota(jnp.int32, (side, side), 0) == lax.broadcasted_iota(jnp.int32, (side, side), 1)
    for b in range(rows // side):
        line = jnp.broadcast_to(gain[:, b * side : (b + 1) * side], (side, side))
        scale = jnp.sum(jnp.where(eye, line, 0.0), axis=1, keepdims=True)
        gcol[b * side : (b + 1) * side, :] = jnp.broadcast_to(scale, (side, 128))

    def convert(k):
        load_up(k).wait()
        for j in range(0, w, 128):
            upb[k, :, j : j + 128] = (gcol[...] * stage[lax.rem(k, depth), :, j : j + 128]).astype(upb.dtype)

        @pl.when(k + depth < pieces)
        def _():
            load_up(k + depth).start()

    def send_parts(k):
        for r in range(n_s):
            x_part(k, r).start()
        for r in range(n_s):
            start_peer(0, k, r * sub, sub)

    def send(k):
        x_copy(k).start()
        start_peer(0, k, 0, rows)

    convert(0)
    pl.semaphore_wait(pltpu.get_barrier_semaphore(), n_fs + 1)

    for k in range(min(m, pieces - 1)):
        convert(k + 1)
        send_parts(k)

    def send_closing(k):
        x_copy(k).start()
        for r in range(n_s):
            start_peer(0, k, r * sub, sub, prf.at[f, r])

    def convert_and_send(k):
        convert(k)
        send(k - 1)

    lax.fori_loop(m + 1, closing + 1 if fine else pieces, lambda k, c: (convert_and_send(k), c)[1], 0)
    for k in range(closing, pieces - 1):
        convert(k + 1)
        send_closing(k)
    pacc[...] = jnp.zeros_like(pacc)
    (send_closing if fine else send if pieces > m else send_parts)(pieces - 1)

    def convert_down(c):
        load_down(c).wait()
        held_down[span(c, d_part), span(t, d_width)] = dstage[lax.rem(c, 2)].astype(held_down.dtype)

        @pl.when(c + 2 < n_c)
        def _():
            load_down(c + 2).start()

    def between(k):
        @pl.when(k == max(pieces - 2, 0))
        def _():
            loop(n_c, lambda c: d_copy(c).start())
            to_near(t).start()

        @pl.when(k < n_c)
        def _():
            convert_down(k)

        @pl.when(k == n_c)
        def _():
            scaled = square_norm(tokens[...].astype(jnp.float32)).astype(jnp.bfloat16)
            for i in range(n_fs):
                normed[i] = scaled[:, i * rows : (i + 1) * rows]

    def pass_parts(k):
        for r in range(n_s):
            x_part(k, r).wait_recv()
            start_peer(1, k, r * sub, sub)
        between(k)

    def pass_on(k):
        x_copy(k).wait_recv()
        start_peer(1, k, 0, rows)
        between(k)

    def pass_closing(k):
        x_copy(k).wait_recv()
        for r in range(n_s):
            start_peer(1, k, r * sub, sub, prf.at[f, r])
        between(k)

    loop(m, pass_parts)
    lax.fori_loop(m, closing, lambda k, c: (pass_on(k), c)[1], 0)
    lax.fori_loop(closing, pieces, lambda k, c: (pass_closing(k), c)[1], 0)

    def gather(c, final):
        def pass_down():
            remote(block(c, far), block(c, far), ds, dr.at[c], {"tp": far}).wait_recv()
            d_pass(c, far).start()

        if not final:
            pass_down()
        acc[...] = jnp.zeros_like(acc)
        mine = f // half

        def source_at(side, step):
            return lax.rem(mine + side, 2) * half + lax.rem(f + step, half)

        def rows_at(first, count):
            return held_up.at[pl.ds(pl.multiple_of(first * rows, rows), count * rows), span(c, w)]

        def side_rows(side):
            return rows_at(lax.rem(mine + side, 2) * half, half)

        def share(src, to, sem):
            return remote(src, to, ws, sem, {"tp": near})

        def share_sem(side, source):
            return wrf.at[source] if final else wr.at[side, c]

        def keep_own(held):
            k = c * m + lax.rem(f, m)
            share(held.at[k], rows_at(f, 1), share_sem(0, f)).start()
            held_up[span(f, rows), span(c, w)] = held[k]

        @pl.when(jnp.logical_and(active, block_of_f == t))
        def _():
            keep_own(upb)

        @pl.when(jnp.logical_and(active, block_of_f != t))
        def _():
            keep_own(xup)

        def pass_part(side, i):
            source, r = source_at(side, lax.rem(i, half)), i // half
            part = landed_part(source, c, r)
            share(part, part, prf.at[source, r]).wait_recv()
            share(part, part, wrf.at[source]).start()

        def add_up(source):
            acc[...] += jnp.dot(
                normed[source], held_up[span(source, rows), span(c, w)], preferred_element_type=jnp.float32
            )

        for side in range(2):
            if final and side == 1:
                pass_down()

            @pl.when(active)
            def _():
                if final:
                    def one(i):
                        @pl.when(jnp.logical_or(side > 0, lax.rem(i, half) > 0))
                        def _():
                            pass_part(side, i)

                    loop(half * n_s, one)
                elif side == 0:
                    others = rows_at(0, half - 1)
                    share(others, others, pr.at[side, c]).wait_recv()

                    def one(i):
                        at = rows_at(source_at(side, i + 1), 1)
                        share(at, at, wr.at[side, c]).start()

                    loop(half - 1, one)
                else:
                    at = side_rows(side)
                    share(at, at, pr.at[side, c]).wait_recv()
                    share(at, at, wr.at[side, c]).start()

            if not final:
                @pl.when(jnp.logical_not(active))
                def _():
                    share(side_rows(side), side_rows(side), wr.at[side, c]).wait_recv()

            def close_one(step):
                source = source_at(side, step)
                if final:
                    @pl.when(jnp.logical_not(active))
                    def _():
                        share(rows_at(source, 1), rows_at(source, 1), wrf.at[source]).wait_recv()

                add_up(source)

            loop(half, close_one)

        hid[...] = jnp.square(jnp.maximum(acc[...], 0.0)).astype(jnp.bfloat16)
        d_pass(c, near_far).wait_recv()

        @pl.when(c == 0)
        def _():
            to_near(near).wait_recv()

    def add_down(c, first, count):
        tile = min(d_width, 512)

        def one(i):
            at = pl.ds(pl.multiple_of(first + i * tile, tile), tile)
            pacc[:, at] += jnp.dot(hid[...], held_down[span(c, d_part), at], preferred_element_type=jnp.float32)

        loop(count // tile, one)

    def whole_chunk(c):
        gather(c, False)
        add_down(c, 0, width)

    last = n_c - 1
    loop(last, whole_chunk)
    gather(last, fine)
    if fused:
        @pl.when(lax.rem(t, 2) == 0)
        def _():
            reduce_rows(pacc, post, out, lambda s, seg: add_down(last, s * seg, seg), False, *reduce_refs)
    else:
        add_down(last, 0, width)
        out[...] = jnp.zeros_like(out)

    @pl.when(active)
    def _():
        remote(held_up, held_up, ws, ws, {"tp": near}).wait_send()

    to_near(t).wait_send()
    remote(column(t), column(t), ds, ds, {"tp": far}).wait_send()
    remote(column(far), column(far), vs, vs, {"tp": near}).wait_send()
    remote(upb, xup, xs, xs, {"tp": far}).wait_send()
    end_peers(0)
    end_peers(1)


def reduce_rows(pacc, post, out, compute, waiting, sb, land, sb2, land2, fin, ss, rs, ss2, rs2):
    f = lax.axis_index("fs")
    _, q, n_o, part, seg = sb.shape
    i, o = lax.rem(f, q), f // q

    def peer(d):
        return lax.rem(i + d, q)

    def across(d):
        return lax.rem(o + d, n_o)

    def first_copy(s, d):
        return remote(sb.at[s, peer(d)], land.at[s, i], ss, rs.at[s], {"fs": o * q + peer(d)})

    def second_copy(s, d):
        return remote(sb2.at[s, across(d)], land2.at[s, o], ss2, rs2.at[s], {"fs": across(d) * q + i})

    ready = SEGMENTS // 2

    def fill(s):
        for b in range(n_o * q):
            sb[s, b % q, b // q] = pacc[b * part : (b + 1) * part, s * seg : (s + 1) * seg].astype(sb.dtype)

    def send(s):
        for d in range(1, q):
            first_copy(s, d).start()

    if waiting:
        for s in range(SEGMENTS):
            compute(s, seg)
            fill(s)
            if s == ready:
                pl.semaphore_wait(pltpu.get_barrier_semaphore(), n_o * q - 1)
                for r in range(s):
                    send(r)
            if s >= ready:
                send(s)
    else:
        for s in range(SEGMENTS):
            compute(s, seg)
            fill(s)
            send(s)

    for s in range(SEGMENTS):
        arrived = land.at[s, pl.ds(0, q - 1)]
        remote(arrived, arrived, ss, rs.at[s], {"fs": f}).wait_recv()

        def total(to):
            value = pacc[span(to * q + i, part), s * seg : (s + 1) * seg]
            for d in range(1, q):
                value += land[s, peer(d), to].astype(jnp.float32)
            return value

        for d in range(1, n_o):
            sb2[s, across(d)] = total(across(d)).astype(sb2.dtype)
        fin[:, s * seg : (s + 1) * seg] = total(o)
        for d in range(1, n_o):
            second_copy(s, d).start()

    for s in range(SEGMENTS):
        value = fin[:, s * seg : (s + 1) * seg]
        arrived = land2.at[s, pl.ds(0, n_o - 1)]
        remote(arrived, arrived, ss2, rs2.at[s], {"fs": f}).wait_recv()
        for d in range(1, n_o):
            value += land2[s, across(d)].astype(jnp.float32)
        fin[:, s * seg : (s + 1) * seg] = value
    summed = fin[...]
    scale = lax.rsqrt(jnp.mean(summed * summed, axis=-1, keepdims=True) + EPS)
    out[...] = (summed * scale * post[...]).astype(out.dtype)
    for buffer, count, sem in ((sb, q - 1, ss), (sb2, n_o - 1, ss2)):
        sent = buffer.at[:, pl.ds(0, count)]
        remote(sent, sent, sem, sem, {"fs": f}).wait_send()


def late_kernel(n_fs, parts, hidden, held_down, post, early, up_token, down_token, out, pacc, *refs):
    f, t = lax.axis_index("fs"), lax.axis_index("tp")

    @pl.when(lax.rem(t, 2) == 1)
    def _():
        loop(n_fs - 1, lambda i: greet({"fs": lax.rem(f + 1 + i, n_fs)}))
        w = hidden.shape[1]
        tile = 512

        def add_last(s, seg):
            for j in range(s * seg, (s + 1) * seg, tile):
                down = held_down[held_down.shape[0] - w :, j : j + tile]
                product = jnp.dot(hidden[...], down, preferred_element_type=jnp.float32)
                pacc[:, j : j + tile] = parts[:, j : j + tile] + product

        reduce_rows(pacc, post, out, add_last, True, *refs)

    @pl.when(lax.rem(t, 2) == 0)
    def _():
        out[...] = early[...]


def store_kernel(src, dst, token, sems):
    count = sems.shape[0]
    size = src.shape[0] // count
    copies = [
        pltpu.make_async_copy(src.at[pl.ds(p * size, size)], dst.at[pl.ds(p * size, size)], sems.at[p])
        for p in range(count)
    ]
    for copy in copies:
        copy.start()
    token[...] = jnp.zeros_like(token)
    for copy in copies:
        copy.wait()


def store(array):
    return pl.pallas_call(
        store_kernel,
        out_shape=(jax.ShapeDtypeStruct(array.shape, array.dtype), jax.ShapeDtypeStruct((8, 128), jnp.float32)),
        in_specs=[pl.BlockSpec(memory_space=pltpu.VMEM)],
        out_specs=(pl.BlockSpec(memory_space=pl.ANY), pl.BlockSpec(memory_space=pltpu.VMEM)),
        scratch_shapes=[pltpu.SemaphoreType.DMA((STORES,))],
        compiler_params=pltpu.CompilerParams(vmem_limit_bytes=1000000),
    )(array)


def sum_kernel(n_fs, parts, gain, out, land, ss, rs):
    f = lax.axis_index("fs")

    def peer_of(i):
        return lax.rem(f + 1 + i, n_fs)

    loop(n_fs - 1, lambda i: greet({"fs": peer_of(i)}))
    pl.semaphore_wait(pltpu.get_barrier_semaphore(), n_fs - 1)

    def send(i):
        return remote(parts.at[peer_of(i)], land.at[f], ss.at[i], rs.at[f], {"fs": peer_of(i)})

    loop(n_fs - 1, lambda i: send(i).start())

    def add(i, total):
        source = peer_of(i)
        remote(land.at[source], land.at[source], ss.at[i], rs.at[source], {"fs": source}).wait_recv()
        return total + land[source].astype(jnp.float32)

    summed = lax.fori_loop(0, n_fs - 1, add, parts[f].astype(jnp.float32))
    scale = lax.rsqrt(jnp.mean(summed * summed, axis=-1, keepdims=True) + EPS)
    out[...] = (summed * scale * gain[...]).astype(out.dtype)
    loop(n_fs - 1, lambda i: send(i).wait_send())


def on_device(n_fs, n_tp, prompt_tokens, trained_up, trained_down, pre_gain, post_gain):
    bf16, f32 = jnp.bfloat16, jnp.float32
    rows, cols = trained_up.shape
    d_rows, d_cols = trained_down.shape
    tokens, width = prompt_tokens.shape[1:]
    m = n_fs // n_tp
    owned = cols // m
    w = min(owned, CHUNK)
    n_c = owned // w
    pieces = m * n_c
    share = tokens // n_fs
    q = GROUP
    n_o = n_fs // q
    seg = width // SEGMENTS
    fused = share % 16 == 0 and n_fs % q == 0 and n_o > 1
    anywhere = pl.BlockSpec(memory_space=pl.ANY)
    vmem = pl.BlockSpec(memory_space=pltpu.VMEM)
    dma = pltpu.SemaphoreType.DMA
    reduce_scratch = [
        pltpu.VMEM((SEGMENTS, q, n_o, share, seg), bf16),
        pltpu.VMEM((SEGMENTS, q, n_o, share, seg), bf16),
        pltpu.VMEM((SEGMENTS, n_o, share, seg), bf16),
        pltpu.VMEM((SEGMENTS, n_o, share, seg), bf16),
        pltpu.VMEM((share, width), f32),
        dma, dma((SEGMENTS,)),
        dma, dma((SEGMENTS,)),
    ]
    held_up, held_down, parts, hidden, early = pl.pallas_call(
        functools.partial(spread_kernel, n_fs, n_tp, w, fused),
        out_shape=(
            pltpu.VMEM((n_fs * rows, owned), bf16),
            pltpu.VMEM((d_rows, n_tp * d_cols), bf16),
            pltpu.VMEM((tokens, width), f32),
            pltpu.VMEM((tokens, w), bf16),
            jax.ShapeDtypeStruct((share, width), bf16),
        ),
        in_specs=[anywhere, anywhere, vmem, vmem, vmem],
        out_specs=(vmem, vmem, vmem, vmem, vmem),
        scratch_shapes=[
            pltpu.VMEM((min(DEPTH, pieces), rows, w), f32),
            pltpu.VMEM((2, d_rows // n_c, d_cols), f32),
            pltpu.VMEM((pieces, rows, w), bf16),
            pltpu.VMEM((pieces, rows, w), bf16),
            pltpu.VMEM((rows, 128), f32),
            pltpu.VMEM((n_fs, tokens, rows), bf16),
            pltpu.VMEM((tokens, w), f32),
            dma((min(DEPTH, pieces),)), dma((2,)),
            dma, dma((pieces + m * (PARTS - 1),)),
            dma((2,)), dma((2, n_c)), dma((n_fs, PARTS)),
            dma, dma((2, n_c)), dma((n_fs,)),
            dma, dma,
            dma, dma((n_c,)),
            dma, dma((n_c,)),
        ] + (reduce_scratch if fused else []),
        compiler_params=pltpu.CompilerParams(collective_id=0, has_side_effects=True, vmem_limit_bytes=30500000),
    )(trained_up, trained_down, prompt_tokens[0], pre_gain[None], post_gain[None])
    sampler_up, up_token = store(held_up)
    sampler_down, down_token = store(held_down)
    if fused:
        layer_out = pl.pallas_call(
            functools.partial(late_kernel, n_fs),
            out_shape=jax.ShapeDtypeStruct((share, width), bf16),
            in_specs=[vmem, vmem, vmem, vmem, vmem, anywhere, anywhere],
            out_specs=vmem,
            scratch_shapes=[pltpu.VMEM((tokens, width), f32)] + reduce_scratch,
            compiler_params=pltpu.CompilerParams(collective_id=1, has_side_effects=True, vmem_limit_bytes=16000000),
        )(parts, hidden, held_down, post_gain[None], early, up_token, down_token)
        return (layer_out[None], sampler_up, sampler_down)

    layer_out = pl.pallas_call(
        functools.partial(sum_kernel, n_fs),
        out_shape=jax.ShapeDtypeStruct((share, width), bf16),
        in_specs=[vmem, vmem],
        out_specs=vmem,
        scratch_shapes=[pltpu.VMEM((n_fs, share, width), bf16), dma((n_fs - 1,)), dma((n_fs,))],
        compiler_params=pltpu.CompilerParams(collective_id=1, has_side_effects=True, vmem_limit_bytes=16000000),
    )(parts.astype(bf16).reshape(n_fs, share, width), post_gain[None])
    return (layer_out[None], sampler_up, sampler_down)


def solution(mesh):
    placed = (P("tp", None, None), P("fs", "tp"), P("fs", "tp"), P("fs"), P())
    return jax.shard_map(
        functools.partial(on_device, mesh.shape["fs"], mesh.shape["tp"]),
        mesh=mesh,
        in_specs=placed,
        out_specs=(P("tp", "fs", None), P(None, "fs"), P("fs", None)),
        check_vma=False,
    )
```
